32 devices in a mesh: sp: 16 (over z, y, core), tp: 2 (over x).
Axes of the slice: x: 2, y: 2, z: 4, core: 2. Of those that a mesh axis runs over, the one named last changes fastest.
Arguments:
- resid: bfloat16 [8192, 2048], P(('sp', 'tp')), may hold values from -3 to 3
- queries: bfloat16 [8192, 1024], P('sp', 'tp'), may hold values from -6 to 6
- keys: bfloat16 [8192, 512], P('sp', 'tp'), may hold values from -6 to 6
- values: bfloat16 [8192, 512], P('sp', 'tp'), may hold values from -6 to 6
- documents: int32 [8192], P('sp'), may hold values from 0 to 7, never falling along the last dimension, each value on 1 to 2048 neighbouring positions
- sinks: float32 [16], P('tp'), may hold values from 0 to 5
- out_proj: bfloat16 [1024, 2048], replicated, may hold values from -0.75 to 0.75
- norm_gain: float32 [2048], replicated, may hold values from 0.1 to 1.9
- gate_proj: bfloat16 [2048, 5632], P('sp', 'tp'), may hold values from -0.125 to 0.125
- up_proj: bfloat16 [2048, 5632], P('sp', 'tp'), may hold values from -0.125 to 0.125
- down_proj: bfloat16 [5632, 2048], P('tp', 'sp'), may hold values from -0.078125 to 0.078125
Outputs:
- mixed: bfloat16 [8192, 2048], P(('sp', 'tp'))
The draws below stay inside these ranges and needn't reach their ends.
Inputs may be any that keep to these rules, and one draw needn't show every extreme that they name: `documents`: document numbers never fall along the sequence; each document holds at most 2048 positions.
All inputs are finite; a program needn't handle non-finite values.
Results may differ from the reference program's by a relative error of at most 0.0095.
Values may be sent and summed in bfloat16 or wider, within the bound.
A program may use at most 128 MiB of HBM per device.

```python
import math
import jax
import jax.numpy as jnp
import numpy as np
from jax import lax

D = 2048
FF = 5632
HEADS = 16
KV_HEADS = 8
HD = 64
WINDOW = 128
TOK_DEV = 512
TOKENS = 8192
DOCS = 8
N_TP = 2


def draw_pair(key):
    base = jax.random.fold_in(key, 17)
    first, second = jax.random.split(base, 2)
    queries = jnp.clip(jax.random.normal(first, (TOKENS, HEADS * HD), jnp.float32), -6.0, 6.0)
    keys = jnp.clip(jax.random.normal(second, (TOKENS, KV_HEADS * HD), jnp.float32), -6.0, 6.0)
    return (queries, keys)


def draw_queries(key, part):
    return draw_pair(key)[0].astype(jnp.bfloat16)


def draw_keys(key, part):
    return draw_pair(key)[1].astype(jnp.bfloat16)


def block_scale(stream_key, dims, cuts, low, top_value):
    loudness, own = 1.0, jax.random.fold_in(stream_key, 6)
    for position, shards_of in cuts:
        steps = jnp.exp(jax.random.uniform(jax.random.fold_in(own, position), (shards_of,), jnp.float32, low / len(cuts), top_value / len(cuts)))
        loudness = loudness * jnp.repeat(steps, dims[position] // shards_of).reshape([-1 if axis == position else 1 for axis in range(len(dims))])
    return loudness


def length_profile(amount, total, limit, skew):
    weights = [(1 << 20) // math.isqrt(rank ** skew) + 1 for rank in range(2, amount + 1)]
    surplus, given = total - limit - (amount - 1), [1] * (amount - 1)
    while surplus > 0:
        candidates = [i for i in range(amount - 1) if given[i] < limit]
        pool, remaining = sum([weights[i] for i in candidates]), surplus
        for i in candidates:
            addition = min(limit - given[i], max(1, remaining * weights[i] // pool), surplus)
            given[i] = given[i] + addition
            surplus = surplus - addition
    return np.array([limit] + given)


def uneven_parts(key, count, total, most, skew):
    if count == 2:
        one = jax.random.randint(key, (), max(1, total - most), min(most, total - 1) + 1)
        return jnp.stack([one, total - one])
    tallies = jnp.asarray(length_profile(count, total, most, skew), jnp.int32)
    twos = (count - 1) // 2
    giver, receiver = tallies[1:1 + 2 * twos:2], tallies[2:2 + 2 * twos:2]
    slack = jnp.minimum(giver - 1, most - receiver)
    shifted = jax.random.randint(jax.random.fold_in(key, 1), (twos,), 0, 1 << 20) % (slack + 1)
    tallies = tallies.at[1:1 + 2 * twos:2].set(giver - shifted).at[2:2 + 2 * twos:2].set(receiver + shifted)
    return tallies[jax.random.permutation(jax.random.fold_in(key, 2), count)]


def noise(key, shape, deviation, limit, cuts=(), held_as=jnp.bfloat16):
    loudness = block_scale(key, shape, cuts, -0.22, 0.18) if cuts else 1.0
    entries = jax.random.normal(key, shape, jnp.float32) * deviation * loudness
    return jnp.minimum(jnp.maximum(entries, -limit), limit).astype(held_as)


def setup_inputs(seed: int = 0) -> dict:
    splits = jax.random.split(jax.random.key(seed), 12)
    resid = noise(splits[0], (TOKENS, D), 0.5, 3.0, ((0, 32),))
    queries = draw_queries(jax.random.fold_in(splits[11], 71), 0)
    keys = draw_keys(jax.random.fold_in(splits[11], 71), 0)
    values = noise(splits[3], (TOKENS, KV_HEADS * HD), 1.0, 6.0, ((0, 16), (1, 2)))
    documents = jnp.searchsorted(jnp.cumsum(uneven_parts(splits[4], DOCS, TOKENS, 4 * TOK_DEV, 0)), jnp.arange(TOKENS), side="right").astype(jnp.int32)
    sinks = jnp.clip(5.0 * jax.random.uniform(splits[5], (HEADS,), jnp.float32) ** block_scale(splits[5], (HEADS,), ((0, 2),), -0.2, 0.2), 0.0, 5.0)
    out_proj = noise(splits[6], (HEADS * HD, D), HD ** -0.5, 0.75)
    norm_gain = jnp.clip(1.0 + 0.18 * jax.random.normal(splits[7], (D,), jnp.float32), 0.1, 1.9)
    gate_proj = noise(splits[8], (D, FF), D ** -0.5, 0.125, ((0, 16), (1, 2)))
    up_proj = noise(splits[9], (D, FF), D ** -0.5, 0.125, ((0, 16), (1, 2)))
    down_proj = noise(splits[10], (FF, D), FF ** -0.5, 0.078125, ((0, 2), (1, 16)))
    return {"resid": resid, "queries": queries, "keys": keys, "values": values, "documents": documents, "sinks": sinks, "out_proj": out_proj, "norm_gain": norm_gain, "gate_proj": gate_proj, "up_proj": up_proj, "down_proj": down_proj}


def band_attend(queries, keys, values, documents, sinks):
    rows = queries.shape[0]
    kv_heads = keys.shape[1] // HD
    group = queries.shape[1] // HD // kv_heads
    blocks = rows // WINDOW
    zero_keys = jnp.zeros((WINDOW, keys.shape[1]), jnp.float32)
    ext_keys = jnp.concatenate([zero_keys, keys.astype(jnp.float32)], axis=0).reshape(blocks + 1, WINDOW, kv_heads, HD)
    ext_values = jnp.concatenate([zero_keys, values.astype(jnp.float32)], axis=0).reshape(blocks + 1, WINDOW, kv_heads, HD)
    ext_docs = jnp.concatenate([jnp.zeros((WINDOW,), jnp.int32), documents.astype(jnp.int32)], axis=0).reshape(blocks + 1, WINDOW)
    band_keys = jnp.concatenate([ext_keys[:-1], ext_keys[1:]], axis=1)
    band_values = jnp.concatenate([ext_values[:-1], ext_values[1:]], axis=1)
    band_docs = jnp.concatenate([ext_docs[:-1], ext_docs[1:]], axis=1)
    query_docs = documents.reshape(blocks, WINDOW)
    distance = jnp.arange(WINDOW)[:, None] + WINDOW - jnp.arange(2 * WINDOW)[None, :]
    key_pos = jnp.arange(blocks)[:, None] * WINDOW + jnp.arange(2 * WINDOW)[None, :] - WINDOW
    visible = ((distance >= 0) & (distance < WINDOW))[None] & (key_pos >= 0)[:, None, :] & (band_docs[:, None, :] == query_docs[:, :, None])
    query_blocks = queries.astype(jnp.float32).reshape(blocks, WINDOW, kv_heads, group, HD)
    scores = jnp.einsum('nikgd,njkd->nkgij', query_blocks, band_keys) * HD ** (-0.5)
    scores = jnp.where(visible[:, None, None], scores, -jnp.inf)
    sink_logit = sinks.astype(jnp.float32).reshape(kv_heads, group)[None, :, :, None, None]
    row_top = jnp.maximum(lax.optimization_barrier(jnp.max(scores, axis=-1, keepdims=True)), sink_logit)
    raw_weights = jnp.exp(scores - row_top)
    totals = lax.optimization_barrier(jnp.sum(raw_weights, axis=-1, keepdims=True)) + jnp.exp(sink_logit - row_top)
    weights = (raw_weights / totals).astype(jnp.bfloat16).astype(jnp.float32)
    attended = jnp.einsum('nkgij,njkd->nikgd', weights, band_values)
    return attended.astype(jnp.bfloat16).reshape(rows, kv_heads * group * HD)

def reference(resid, queries, keys, values, documents, sinks, out_proj, norm_gain, gate_proj, up_proj, down_proj):
    group = HEADS // KV_HEADS
    pieces = []
    for head in range(KV_HEADS):
        pieces.append(band_attend(queries[:, head * group * HD:(head + 1) * group * HD], keys[:, head * HD:(head + 1) * HD], values[:, head * HD:(head + 1) * HD], documents, sinks[head * group:(head + 1) * group]))
    attended = jnp.concatenate(pieces, axis=1)
    mid_rows = resid.astype(jnp.float32) + jnp.dot(attended, out_proj, preferred_element_type=jnp.float32)
    scale = lax.rsqrt(lax.optimization_barrier(jnp.mean(mid_rows * mid_rows, axis=-1, keepdims=True)) + 1e-06)
    normed = (mid_rows * scale * norm_gain).astype(jnp.bfloat16)
    width = FF // N_TP

    def ffn_rows(row_block):
        gate_acts = jnp.dot(row_block, gate_proj, preferred_element_type=jnp.float32)
        up_acts = jnp.dot(row_block, up_proj, preferred_element_type=jnp.float32)
        hidden = (jax.nn.silu(gate_acts) * up_acts).astype(jnp.bfloat16)
        totals = jnp.zeros((row_block.shape[0], D), jnp.float32)
        for block in range(N_TP):
            partial_value = jnp.dot(hidden[:, block * width:(block + 1) * width], down_proj[block * width:(block + 1) * width], preferred_element_type=jnp.float32).astype(jnp.bfloat16)
            totals = totals + lax.optimization_barrier(partial_value).astype(jnp.float32)
        return totals
    summed = lax.map(ffn_rows, normed.reshape(TOKENS // TOK_DEV, TOK_DEV, D)).reshape(TOKENS, D)
    return (mid_rows + summed).astype(jnp.bfloat16)
```

```python
import jax
import jax.numpy as jnp
from jax import lax
from jax.experimental import pallas as pl
from jax.experimental.pallas import tpu as pltpu
from jax.sharding import PartitionSpec as P

HD = 64
WINDOW = 128
SHARE = 4


def passed_along(value, axis, steps):
    count = lax.axis_size(axis)
    first, last = (max(0, -steps), min(count, count - steps))
    return lax.ppermute(value, axis, [(source, source + steps) for source in range(first, last)])


def swapped(value, axis, mask):
    count = lax.axis_size(axis)
    return lax.ppermute(value, axis, [(source, source ^ mask) for source in range(count)])


def bits_of(count):
    return [1 << bit for bit in range(count.bit_length() - 1)]


def attend(queries, keys, values, documents, sinks):
    rows = queries.shape[0]
    kv_heads = keys.shape[1] // HD
    group = queries.shape[1] // HD // kv_heads
    blocks = rows // WINDOW
    key_value = jnp.concatenate([keys, values], axis=1)
    tail_pair, tail_docs = passed_along(
        (key_value[rows - WINDOW :], documents[rows - WINDOW :].astype(jnp.bfloat16)), "sp", 1
    )
    ext_pair = jnp.concatenate([tail_pair, key_value], axis=0).reshape(
        blocks + 1, WINDOW, 2 * kv_heads * HD
    )
    ext_docs = jnp.concatenate([tail_docs.astype(jnp.int32), documents], axis=0).reshape(
        blocks + 1, WINDOW
    )
    band = jnp.concatenate([ext_pair[:-1], ext_pair[1:]], axis=1)
    band_keys = band[:, :, : kv_heads * HD].reshape(blocks, 2 * WINDOW, kv_heads, HD)
    band_values = band[:, :, kv_heads * HD :].reshape(blocks, 2 * WINDOW, kv_heads, HD)
    band_docs = jnp.concatenate([ext_docs[:-1], ext_docs[1:]], axis=1)
    query_docs = documents.reshape(blocks, WINDOW)
    offset = lax.axis_index("sp") * rows
    distance = jnp.arange(WINDOW)[:, None] + WINDOW - jnp.arange(2 * WINDOW)[None, :]
    key_pos = (
        offset + jnp.arange(blocks)[:, None] * WINDOW + jnp.arange(2 * WINDOW)[None, :] - WINDOW
    )
    visible = (
        ((distance >= 0) & (distance < WINDOW))[None]
        & (key_pos >= 0)[:, None, :]
        & (band_docs[:, None, :] == query_docs[:, :, None])
    )
    query_blocks = queries.reshape(blocks, WINDOW, kv_heads, group, HD)
    scores = jnp.einsum(
        "nikgd,njkd->nkgij", query_blocks, band_keys, preferred_element_type=jnp.float32
    ) * HD ** (-0.5)
    scores = jnp.where(visible[:, None, None], scores, -jnp.inf)
    sink_logit = sinks.reshape(kv_heads, group)[None, :, :, None, None]
    row_top = jnp.maximum(jnp.max(scores, axis=-1, keepdims=True), sink_logit)
    raw_weights = jnp.exp(scores - row_top)
    totals = jnp.sum(raw_weights, axis=-1, keepdims=True) + jnp.exp(sink_logit - row_top)
    weights = (raw_weights / totals).astype(jnp.bfloat16)
    attended = jnp.einsum(
        "nkgij,njkd->nikgd", weights, band_values, preferred_element_type=jnp.float32
    )
    return attended.astype(jnp.bfloat16).reshape(rows, kv_heads * group * HD)


def norm_rows(mid_rows, norm_gain):
    scale = lax.rsqrt(jnp.mean(mid_rows * mid_rows, axis=-1, keepdims=True) + 1e-06)
    return (mid_rows * scale * norm_gain).astype(jnp.bfloat16)


def by_place(pieces, me):
    for bit in bits_of(len(pieces)):
        flip = (me & bit) != 0
        pieces = [jnp.where(flip, pieces[r ^ bit], pieces[r]) for r in range(len(pieces))]
    return pieces


def own_rows(attended):
    count = lax.axis_size("tp")
    me = lax.axis_index("tp")
    rows = attended.shape[0] // count
    pieces = []
    for mask in range(count):
        piece = lax.dynamic_slice_in_dim(attended, (me ^ mask) * rows, rows)
        pieces.append(swapped(piece, "tp", mask) if mask else piece)
    return jnp.concatenate(by_place(pieces, me), axis=1)


def regrouped(gate_proj, up_proj, down_proj):
    me = lax.axis_index("sp") % SHARE
    width = gate_proj.shape[1] // SHARE
    gate_up, down = [], []
    for mask in range(SHARE):
        start = (me ^ mask) * width
        piece = jnp.concatenate(
            [
                lax.dynamic_slice_in_dim(gate_proj, start, width, axis=1),
                lax.dynamic_slice_in_dim(up_proj, start, width, axis=1),
            ],
            axis=1,
        )
        gate_up.append(swapped(piece, "sp", mask) if mask else piece)
    for mask in range(SHARE):
        piece = lax.dynamic_slice_in_dim(down_proj, (me ^ mask) * width, width, axis=0)
        down.append(swapped(piece, "sp", mask) if mask else piece)
    return (
        jnp.concatenate(by_place(gate_up, me), axis=0),
        jnp.concatenate(by_place(down, me), axis=1),
    )


def spread(chunk):
    groups = lax.axis_size("sp") // SHARE
    if groups == 4:
        half = chunk.shape[0] // 2
        low = swapped(chunk, "sp", SHARE)
        wrap = swapped(chunk, "sp", 3 * SHARE)
        first = swapped(low[:half], "sp", 3 * SHARE)
        second = swapped(wrap[half:], "sp", SHARE)
        return [chunk, low, jnp.concatenate([first, second], axis=0), wrap]
    chunks = [chunk]
    for bit in bits_of(groups):
        chunks = chunks + [swapped(piece, "sp", SHARE * bit) for piece in chunks]
    return chunks


def gathered(rows, hops):
    for axis, mask in hops:
        rows = jnp.concatenate([rows, swapped(rows, axis, mask)], axis=0)
    return rows


def scattered(partial, hops):
    total = partial
    for axis, mask in reversed(hops):
        half = total.shape[0] // 2
        arrived = swapped(total[half:].astype(jnp.bfloat16), axis, mask)
        total = total[:half].astype(jnp.float32) + arrived.astype(jnp.float32)
    return total


def shards(
    resid,
    queries,
    keys,
    values,
    documents,
    sinks,
    out_proj,
    norm_gain,
    gate_proj,
    up_proj,
    down_proj,
):
    groups = lax.axis_size("sp") // SHARE
    group = lax.axis_index("sp") // SHARE
    gate_up, down = regrouped(gate_proj, up_proj, down_proj)
    gate_up = jnp.concatenate(spread(gate_up), axis=0)
    down = jnp.concatenate(spread(down), axis=1)
    units = down.shape[0]

    attended = attend(queries, keys, values, documents, sinks)
    mid_rows = resid.astype(jnp.float32) + jnp.dot(
        own_rows(attended), out_proj, preferred_element_type=jnp.float32
    )
    normed = norm_rows(mid_rows, norm_gain)
    rows, width = normed.shape
    block = width // groups
    normed = jnp.concatenate(
        [lax.dynamic_slice_in_dim(normed, (group ^ k) * block, block, axis=1) for k in range(groups)],
        axis=1,
    )
    x_hops = [("tp", bit) for bit in bits_of(lax.axis_size("tp"))]
    y_hops = [("sp", 2)]
    core_hops = [("sp", 1)]
    sums = []
    for stream, hops in enumerate((x_hops + y_hops + core_hops, y_hops + x_hops + core_hops)):
        part = normed[stream * rows // 2 : (stream + 1) * rows // 2]
        part = gathered(part, hops)
        acts = jnp.dot(part, gate_up, preferred_element_type=jnp.float32)
        hidden = (jax.nn.silu(acts[:, :units]) * acts[:, units:]).astype(jnp.bfloat16)
        partial = jnp.dot(hidden, down, preferred_element_type=jnp.float32).astype(jnp.bfloat16)
        sums.append(scattered(partial, hops))
    summed = jnp.concatenate(sums, axis=0)
    stack = jnp.stack([summed[:, k * block : (k + 1) * block] for k in range(groups)])
    summed = jnp.concatenate(
        [lax.dynamic_index_in_dim(stack, group ^ k, keepdims=False) for k in range(groups)], axis=1
    )
    return (mid_rows + summed).astype(jnp.bfloat16)


MESH = pl.DeviceIdType.MESH
CHAIN, SIDE, CORES = 4, 2, 2


def fits(mesh):
    return mesh.shape["sp"] == CHAIN * SIDE * CORES and mesh.shape["tp"] == 2


def layer_kernel(
    documents_ref,
    gain_ref,
    sinks_ref,
    resid_hbm,
    queries_hbm,
    keys_hbm,
    values_hbm,
    out_proj_hbm,
    gate_hbm,
    up_hbm,
    down_hbm,
    out_ref,
    q_v,
    k_v,
    v_v,
    halo_docs,
    resid_v,
    out_proj_v,
    att,
    att_out,
    mid,
    tok,
    gu,
    dn,
    acts,
    hid,
    part,
    x_out,
    x_in,
    z_out,
    z_in,
    local_sem,
    halo_s,
    halo_r,
    own_s,
    own_r,
    tok_s,
    tok_r,
    wl,
    wz_s,
    wz_r,
    wy_s,
    wy_r,
    wc_s,
    wc_r,
    rx_s,
    rx_r,
    rz_s,
    rz_r,
):
    sp = lax.axis_index("sp")
    x = lax.axis_index("tp")
    z = sp // (SIDE * CORES)
    y = (sp // CORES) % SIDE
    c = sp % CORES
    hi, lo = z // 2, z % 2
    pair = z + 1 - 2 * lo
    far_mid = 2 - hi
    far_end = 3 - 3 * hi
    is_mid = jnp.where((z == 1) | (z == 2), 1, 0)

    def at(zz, yy, cc, xx):
        return ((zz * SIDE + yy) * CORES + cc, xx)

    to_pair, to_mid, to_end = at(pair, y, c, x), at(far_mid, y, c, x), at(far_end, y, c, x)
    to_y, to_c, to_x = at(z, 1 - y, c, x), at(z, y, 1 - c, x), (sp, 1 - x)
    count = CHAIN * SIDE * CORES
    to_next = (lax.rem(sp + 1, count), x)
    to_prev = (lax.rem(sp + count - 1, count), x)

    rows, own = q_v.shape[0], resid_v.shape[0]
    depth = gate_hbm.shape[0]
    units = gu.shape[2]
    width = mid.shape[1]
    heads = sinks_ref.shape[0]
    kv_heads = k_v.shape[1] // HD
    group = heads // kv_heads
    blocks = rows // WINDOW
    pane = dn.shape[2]
    cols = heads * HD

    def remote(src, dst, send, recv, device):
        return pltpu.make_async_remote_copy(
            src_ref=src, dst_ref=dst, send_sem=send, recv_sem=recv, device_id=device, device_id_type=MESH
        )

    fetch = [
        pltpu.make_async_copy(queries_hbm, q_v, local_sem.at[0]),
        pltpu.make_async_copy(keys_hbm, k_v.at[pl.ds(WINDOW, rows), :], local_sem.at[1]),
        pltpu.make_async_copy(values_hbm, v_v.at[pl.ds(WINDOW, rows), :], local_sem.at[2]),
        pltpu.make_async_copy(resid_hbm, resid_v, local_sem.at[3]),
        pltpu.make_async_copy(out_proj_hbm, out_proj_v, local_sem.at[4]),
    ]
    for copy in fetch:
        copy.start()

    barrier = pltpu.get_barrier_semaphore()
    around = (to_pair, to_mid, to_end, to_y, to_c, to_x, to_next, to_prev)
    for device in around:
        pl.semaphore_signal(barrier, inc=1, device_id=device, device_id_type=MESH)
    pl.semaphore_wait(barrier, len(around))

    last = pl.ds(rows - WINDOW, WINDOW)
    halo = [
        remote(keys_hbm.at[last, :], k_v.at[pl.ds(0, WINDOW), :], halo_s.at[0], halo_r.at[0], to_next),
        remote(values_hbm.at[last, :], v_v.at[pl.ds(0, WINDOW), :], halo_s.at[1], halo_r.at[1], to_next),
        remote(documents_ref.at[pl.ds(blocks - 1, 1), :], halo_docs, halo_s.at[2], halo_r.at[2], to_next),
    ]
    for copy in halo:
        copy.start()

    z_of = (z, pair, far_mid, far_end)

    def place(kind, zz, yy, cc):
        if kind == 2:
            return dn.at[zz * SIDE + yy, :, pl.ds(pl.multiple_of(cc * depth, depth), depth)]
        source = (zz * SIDE + yy) * CORES + cc
        return gu.at[kind, pl.ds(pl.multiple_of(source * depth, depth), depth), :]

    def shard(kind, half):
        start = pl.ds(pl.multiple_of(half * units, WINDOW), units)
        if kind == 2:
            return down_hbm.at[start, :]
        return (gate_hbm, up_hbm)[kind].at[:, start]

    def z_send(kind, dest):
        half, device, slot = (
            (1 - lo, to_pair, 0),
            (hi, to_mid, 2 - is_mid),
            (1 - hi, to_end, 2 - is_mid),
        )[dest]
        return remote(
            shard(kind, half), place(kind, z, y, c), wz_s.at[dest, kind], wz_r.at[slot, kind], device
        )

    def z_arrival(kind, slot):
        where = place(kind, z_of[slot], y, c)
        return remote(where, where, wz_s.at[slot - 1, kind], wz_r.at[slot - 1, kind], to_pair)

    def y_send(kind, slot):
        where = place(kind, z_of[slot], y, c)
        return remote(
            shard(kind, lo) if slot == 0 else where, where, wy_s.at[slot, kind], wy_r.at[slot, kind], to_y
        )

    def y_arrival(kind, slot):
        where = place(kind, z_of[slot], 1 - y, c)
        return remote(where, where, wy_s.at[slot, kind], wy_r.at[slot, kind], to_y)

    def c_send(kind, slot, other):
        where = place(kind, z_of[slot], 1 - y if other else y, c)
        source = shard(kind, lo) if slot == 0 and not other else where
        return remote(source, where, wc_s.at[slot, other, kind], wc_r.at[slot, other, kind], to_c)

    def c_arrival(kind, slot, other):
        where = place(kind, z_of[slot], 1 - y if other else y, 1 - c)
        return remote(where, where, wc_s.at[slot, other, kind], wc_r.at[slot, other, kind], to_c)

    kept = [
        pltpu.make_async_copy(shard(kind, lo), place(kind, z, y, c), wl.at[kind]) for kind in range(3)
    ]

    def z_in_and_on(kind, slot):
        z_arrival(kind, slot).wait_recv()
        y_send(kind, slot).start()
        c_send(kind, slot, 0).start()

    def y_in_and_on(kind, slot):
        y_arrival(kind, slot).wait_recv()
        c_send(kind, slot, 1).start()

    for kind in (0, 1):
        z_send(kind, 0).start()
        y_send(kind, 0).start()
        c_send(kind, 0, 0).start()
    y_send(2, 0).start()
    c_send(2, 0, 0).start()

    @pl.when(is_mid == 1)
    def _():
        for kind in (0, 1):
            z_send(kind, 1).start()
            z_send(kind, 2).start()

    for copy in kept:
        copy.start()

    for copy in fetch[:3]:
        copy.wait()
    for copy in halo:
        copy.wait_recv()

    row = lax.broadcasted_iota(jnp.int32, (WINDOW, 2 * WINDOW), 0)
    col = lax.broadcasted_iota(jnp.int32, (WINDOW, 2 * WINDOW), 1)
    distance = row + WINDOW - col
    in_window = (distance >= 0) & (distance < WINDOW)

    def attend_block(block, target, target_row, target_col):
        here = documents_ref[pl.ds(block, 1), :]
        back = documents_ref[pl.ds(jnp.maximum(block - 1, 0), 1), :]
        back = jnp.where(block == 0, halo_docs[...], back)
        band = jnp.concatenate([back, here], axis=1).astype(jnp.float32)
        mine = jnp.broadcast_to(here.astype(jnp.float32), (WINDOW, WINDOW)).T
        mine = jnp.concatenate([mine, mine], axis=1)
        first = jnp.where((sp == 0) & (block == 0), WINDOW, 0)
        visible = in_window & (band == mine) & (col >= first)
        start = pl.multiple_of(block * WINDOW, WINDOW)
        for kv in range(kv_heads):
            k_band = k_v[pl.ds(start, 2 * WINDOW), kv * HD : (kv + 1) * HD]
            v_band = v_v[pl.ds(start, 2 * WINDOW), kv * HD : (kv + 1) * HD]
            pieces = []
            for head in range(kv * group, (kv + 1) * group):
                q = q_v[pl.ds(start, WINDOW), head * HD : (head + 1) * HD]
                scores = lax.dot_general(
                    q, k_band, (((1,), (1,)), ((), ())), preferred_element_type=jnp.float32
                ) * HD ** (-0.5)
                scores = jnp.where(visible, scores, -jnp.inf)
                sink = sinks_ref[head]
                top = jnp.maximum(jnp.max(scores, axis=1, keepdims=True), sink)
                raw = jnp.exp(scores - top)
                total = jnp.sum(raw, axis=1, keepdims=True) + jnp.exp(sink - top)
                weights = (raw / total).astype(jnp.bfloat16)
                pieces.append(jnp.dot(weights, v_band, preferred_element_type=jnp.float32))
            merged = jnp.concatenate(pieces, axis=1).astype(jnp.bfloat16)
            at_col = target_col + kv * group * HD
            if not isinstance(at_col, int):
                at_col = pl.multiple_of(at_col, WINDOW)
            target[pl.ds(target_row, WINDOW), pl.ds(at_col, group * HD)] = merged

    own_blocks = own // WINDOW
    my_cols = pl.ds(pl.multiple_of(x * cols, WINDOW), cols)

    def own_send(part_index):
        part_rows = pl.ds(part_index * WINDOW, WINDOW)
        return remote(
            att_out.at[part_rows, :],
            att.at[part_rows, my_cols],
            own_s.at[part_index],
            own_r.at[part_index],
            to_x,
        )

    for b in range(own_blocks):
        attend_block((1 - x) * own_blocks + b, att_out, b * WINDOW, 0)
        own_send(b).start()
    for b in range(own_blocks):
        attend_block(x * own_blocks + b, att, b * WINDOW, x * cols)

    their_cols = pl.ds(pl.multiple_of((1 - x) * cols, WINDOW), cols)
    for copy in fetch[3:]:
        copy.wait()
    for b in range(own_blocks):
        where = att.at[pl.ds(b * WINDOW, WINDOW), their_cols]
        remote(where, where, own_s.at[b], own_r.at[b], to_x).wait_recv()

    square = jnp.zeros((own, 1), jnp.float32)
    step = 2 * pane
    for n in range(width // step):
        block_cols = pl.ds(n * step, step)
        value = resid_v[:, block_cols].astype(jnp.float32) + jnp.dot(
            att[...], out_proj_v[:, block_cols], preferred_element_type=jnp.float32
        )
        mid[:, block_cols] = value
        square = square + jnp.sum(value * value, axis=1, keepdims=True)
    scale = lax.rsqrt(square * (1.0 / width) + 1e-06)
    for n in range(width // step):
        block_cols = pl.ds(n * step, step)
        tok[pl.ds(0, own), block_cols] = (mid[:, block_cols] * scale * gain_ref[:, block_cols]).astype(
            jnp.bfloat16
        )

    def tok_at(slot):
        return tok.at[pl.ds(slot * own, own), :]

    tok_z = remote(tok_at(0), tok_at(1), tok_s.at[0], tok_r.at[0], to_pair)
    tok_x = remote(tok_at(0), tok_at(2), tok_s.at[1], tok_r.at[1], to_x)
    tok_on = remote(tok_at(1), tok_at(3), tok_s.at[2], tok_r.at[2], to_x)
    tok_z.start()
    tok_x.start()

    @pl.when(is_mid == 0)
    def _():
        for kind in (0, 1, 2):
            z_send(kind, 2).start()
            z_send(kind, 1).start()
        z_send(2, 0).start()

    def ready(kind, slot):
        c_arrival(kind, slot, 0).wait_recv()
        c_arrival(kind, slot, 1).wait_recv()

    tall = own * 4

    def gate_up(slot, first, final):
        deep = pl.ds(pl.multiple_of(z_of[slot] * SIDE * CORES * depth, depth), SIDE * CORES * depth)

        def tile(start, size):
            at_units = pl.ds(start, size)
            sums = []
            for kind in (0, 1):
                value = jnp.dot(tok[:, deep], gu[kind, deep, at_units], preferred_element_type=jnp.float32)
                if not first:
                    value = value + acts[kind, :, at_units]
                if not final:
                    acts[kind, :, at_units] = value
                sums.append(value)
            if final:
                gate_acts, up_acts = sums
                hid[:, at_units] = (gate_acts / (1.0 + jnp.exp(-gate_acts)) * up_acts).astype(jnp.bfloat16)

        whole = units // pane

        def body(n, carry):
            tile(pl.multiple_of(n * pane, pane), pane)
            return carry

        lax.fori_loop(0, whole, body, 0)
        if units % pane:
            tile(whole * pane, units % pane)

    z_in_and_on(0, 1)
    z_in_and_on(1, 1)
    y_in_and_on(0, 0)
    y_in_and_on(1, 0)
    y_in_and_on(2, 0)
    y_in_and_on(0, 1)
    tok_z.wait_recv()
    tok_on.start()
    y_in_and_on(1, 1)
    z_in_and_on(0, 2)
    z_in_and_on(1, 2)
    y_in_and_on(0, 2)
    tok_x.wait_recv()
    tok_on.wait_recv()
    kept[0].wait()
    kept[1].wait()
    ready(0, 0)
    ready(1, 0)
    gate_up(0, True, False)
    y_in_and_on(1, 2)
    z_in_and_on(0, 3)

    @pl.when(is_mid == 1)
    def _():
        for dest in (1, 2, 0):
            z_send(2, dest).start()

    ready(0, 1)
    ready(1, 1)
    gate_up(1, False, False)
    z_in_and_on(1, 3)
    ready(0, 2)
    ready(1, 2)
    gate_up(2, False, False)
    y_in_and_on(0, 3)
    z_in_and_on(2, 1)
    y_in_and_on(1, 3)
    ready(0, 3)
    ready(1, 3)
    gate_up(3, False, True)
    y_in_and_on(2, 1)
    kept[2].wait()

    half = tall // 2
    panes = [(slot, other) for slot in range(4) for other in range(2)]

    def pane_of(i):
        slot, other = panes[i]
        return z_of[slot] * SIDE + (1 - y if other else y)

    def x_sum(i):
        j = pane_of(i)
        return remote(x_out.at[j], x_in.at[j], rx_s.at[i], rx_r.at[i], to_x)

    def down_pane(i):
        j = pane_of(i)
        partial = jnp.dot(hid[...], dn[j], preferred_element_type=jnp.float32)
        x_out[j] = partial[half:, :].astype(jnp.bfloat16)
        part[j] = partial[:half, :]
        x_sum(i).start()

    def z_copy(j):
        return remote(z_out.at[j], z_in.at[j], rz_s.at[j], rz_r.at[j], to_pair)

    def fold(i):
        j = pane_of(i)
        x_sum(i).wait_recv()
        total = part[j] + x_in[j].astype(jnp.float32)
        z_out[j] = total[own:, :].astype(jnp.bfloat16)
        z_copy(j).start()
        part[j, pl.ds(0, own), :] = total[:own, :]

    def finish(i):
        j = pane_of(i)
        z_copy(j).wait_recv()
        at_cols = pl.ds(pl.multiple_of(j * pane, pane), pane)
        out_ref[:, at_cols] = (
            mid[:, at_cols] + (part[j, pl.ds(0, own), :] + z_in[j].astype(jnp.float32))
        ).astype(jnp.bfloat16)

    ready(2, 0)
    down_pane(0)
    down_pane(1)
    ready(2, 1)
    down_pane(2)
    down_pane(3)
    z_in_and_on(2, 2)
    fold(0)
    y_in_and_on(2, 2)
    fold(1)
    ready(2, 2)
    down_pane(4)
    down_pane(5)
    fold(2)
    z_in_and_on(2, 3)
    fold(3)
    y_in_and_on(2, 3)
    fold(4)
    ready(2, 3)
    down_pane(6)
    down_pane(7)
    fold(5)
    for i in range(4):
        finish(i)
    fold(6)
    fold(7)
    for i in range(4, 8):
        finish(i)

    for copy in halo:
        copy.wait_send()
    for b in range(own_blocks):
        own_send(b).wait_send()
    for copy in (tok_z, tok_x, tok_on):
        copy.wait_send()
    for kind in range(3):
        for dest in range(3):
            z_send(kind, dest).wait_send()
        for slot in range(4):
            y_send(kind, slot).wait_send()
            for other in range(2):
                c_send(kind, slot, other).wait_send()
    for i in range(8):
        x_sum(i).wait_send()
        z_copy(pane_of(i)).wait_send()


def one_kernel(
    resid, queries, keys, values, documents, sinks, out_proj, norm_gain, gate_proj, up_proj, down_proj
):
    rows, own, width = queries.shape[0], resid.shape[0], resid.shape[1]
    units = gate_proj.shape[1] // 2
    deep = gate_proj.shape[0] * CHAIN * SIDE * CORES
    pane = gate_proj.shape[0] * CORES
    panes = width // pane
    heads_cols, kv_cols = queries.shape[1], keys.shape[1]
    bf16, f32 = jnp.bfloat16, jnp.float32
    vmem = pl.BlockSpec(memory_space=pltpu.VMEM)
    anywhere = pl.BlockSpec(memory_space=pl.ANY)
    dma = pltpu.SemaphoreType.DMA
    tall = 4 * own
    return pl.pallas_call(
        layer_kernel,
        out_shape=jax.ShapeDtypeStruct((own, width), bf16),
        in_specs=[vmem, vmem, pl.BlockSpec(memory_space=pltpu.SMEM)] + [anywhere] * 8,
        out_specs=vmem,
        scratch_shapes=[
            pltpu.VMEM((rows, heads_cols), bf16),
            pltpu.VMEM((rows + WINDOW, kv_cols), bf16),
            pltpu.VMEM((rows + WINDOW, kv_cols), bf16),
            pltpu.VMEM((1, WINDOW), jnp.int32),
            pltpu.VMEM((own, width), bf16),
            pltpu.VMEM(out_proj.shape, bf16),
            pltpu.VMEM((own, out_proj.shape[0]), bf16),
            pltpu.VMEM((own, heads_cols), bf16),
            pltpu.VMEM((own, width), f32),
            pltpu.VMEM((tall, width), bf16),
            pltpu.VMEM((2, deep, units), bf16),
            pltpu.VMEM((panes, units, pane), bf16),
            pltpu.VMEM((2, tall, units), f32),
            pltpu.VMEM((tall, units), bf16),
            pltpu.VMEM((panes, tall // 2, pane), f32),
            pltpu.VMEM((panes, tall // 2, pane), bf16),
            pltpu.VMEM((panes, tall // 2, pane), bf16),
            pltpu.VMEM((panes, own, pane), bf16),
            pltpu.VMEM((panes, own, pane), bf16),
            dma((5,)),
            dma((3,)),
            dma((3,)),
            dma((own // WINDOW,)),
            dma((own // WINDOW,)),
            dma((3,)),
            dma((3,)),
            dma((3,)),
            dma((3, 3)),
            dma((3, 3)),
            dma((4, 3)),
            dma((4, 3)),
            dma((4, 2, 3)),
            dma((4, 2, 3)),
            dma((panes,)),
            dma((panes,)),
            dma((panes,)),
            dma((panes,)),
        ],
        compiler_params=pltpu.CompilerParams(
            collective_id=0, has_side_effects=True, vmem_limit_bytes=66_000_000
        ),
        name="layer",
    )(
        documents.reshape(rows // WINDOW, WINDOW),
        norm_gain.reshape(1, width),
        sinks,
        resid,
        queries,
        keys,
        values,
        out_proj,
        gate_proj,
        up_proj,
        down_proj,
    )


def solution(mesh):
    in_specs = (
        P(("sp", "tp"), None),
        P("sp", "tp"),
        P("sp", "tp"),
        P("sp", "tp"),
        P("sp"),
        P("tp"),
        P(),
        P(),
        P("sp", "tp"),
        P("sp", "tp"),
        P("tp", "sp"),
    )
    out_specs = P(("sp", "tp"), None)
    if fits(mesh):
        program = lambda *arrays: one_kernel(*arrays)
        return jax.shard_map(
            program, mesh=mesh, in_specs=in_specs, out_specs=out_specs, check_vma=False
        )
    return jax.shard_map(shards, mesh=mesh, in_specs=in_specs, out_specs=out_specs, check_vma=False)
```

```python
import jax
import jax.numpy as jnp
from jax import lax
from jax.experimental import pallas as pl
from jax.experimental.pallas import tpu as pltpu
from jax.sharding import PartitionSpec as P

HD = 64
WINDOW = 128
SHARE = 4


def passed_along(value, axis, steps):
    count = lax.axis_size(axis)
    first, last = (max(0, -steps), min(count, count - steps))
    return lax.ppermute(value, axis, [(source, source + steps) for source in range(first, last)])


def swapped(value, axis, mask):
    count = lax.axis_size(axis)
    return lax.ppermute(value, axis, [(source, source ^ mask) for source in range(count)])


def bits_of(count):
    return [1 << bit for bit in range(count.bit_length() - 1)]


def attend(queries, keys, values, documents, sinks):
    rows = queries.shape[0]
    kv_heads = keys.shape[1] // HD
    group = queries.shape[1] // HD // kv_heads
    blocks = rows // WINDOW
    key_value = jnp.concatenate([keys, values], axis=1)
    tail_pair, tail_docs = passed_along(
        (key_value[rows - WINDOW :], documents[rows - WINDOW :].astype(jnp.bfloat16)), "sp", 1
    )
    ext_pair = jnp.concatenate([tail_pair, key_value], axis=0).reshape(
        blocks + 1, WINDOW, 2 * kv_heads * HD
    )
    ext_docs = jnp.concatenate([tail_docs.astype(jnp.int32), documents], axis=0).reshape(
        blocks + 1, WINDOW
    )
    band = jnp.concatenate([ext_pair[:-1], ext_pair[1:]], axis=1)
    band_keys = band[:, :, : kv_heads * HD].reshape(blocks, 2 * WINDOW, kv_heads, HD)
    band_values = band[:, :, kv_heads * HD :].reshape(blocks, 2 * WINDOW, kv_heads, HD)
    band_docs = jnp.concatenate([ext_docs[:-1], ext_docs[1:]], axis=1)
    query_docs = documents.reshape(blocks, WINDOW)
    offset = lax.axis_index("sp") * rows
    distance = jnp.arange(WINDOW)[:, None] + WINDOW - jnp.arange(2 * WINDOW)[None, :]
    key_pos = (
        offset + jnp.arange(blocks)[:, None] * WINDOW + jnp.arange(2 * WINDOW)[None, :] - WINDOW
    )
    visible = (
        ((distance >= 0) & (distance < WINDOW))[None]
        & (key_pos >= 0)[:, None, :]
        & (band_docs[:, None, :] == query_docs[:, :, None])
    )
    query_blocks = queries.reshape(blocks, WINDOW, kv_heads, group, HD)
    scores = jnp.einsum(
        "nikgd,njkd->nkgij", query_blocks, band_keys, preferred_element_type=jnp.float32
    ) * HD ** (-0.5)
    scores = jnp.where(visible[:, None, None], scores, -jnp.inf)
    sink_logit = sinks.reshape(kv_heads, group)[None, :, :, None, None]
    row_top = jnp.maximum(jnp.max(scores, axis=-1, keepdims=True), sink_logit)
    raw_weights = jnp.exp(scores - row_top)
    totals = jnp.sum(raw_weights, axis=-1, keepdims=True) + jnp.exp(sink_logit - row_top)
    weights = (raw_weights / totals).astype(jnp.bfloat16)
    attended = jnp.einsum(
        "nkgij,njkd->nikgd", weights, band_values, preferred_element_type=jnp.float32
    )
    return attended.astype(jnp.bfloat16).reshape(rows, kv_heads * group * HD)


def norm_rows(mid_rows, norm_gain):
    scale = lax.rsqrt(jnp.mean(mid_rows * mid_rows, axis=-1, keepdims=True) + 1e-06)
    return (mid_rows * scale * norm_gain).astype(jnp.bfloat16)


def by_place(pieces, me):
    for bit in bits_of(len(pieces)):
        flip = (me & bit) != 0
        pieces = [jnp.where(flip, pieces[r ^ bit], pieces[r]) for r in range(len(pieces))]
    return pieces


def own_rows(attended):
    count = lax.axis_size("tp")
    me = lax.axis_index("tp")
    rows = attended.shape[0] // count
    pieces = []
    for mask in range(count):
        piece = lax.dynamic_slice_in_dim(attended, (me ^ mask) * rows, rows)
        pieces.append(swapped(piece, "tp", mask) if mask else piece)
    return jnp.concatenate(by_place(pieces, me), axis=1)


def regrouped(gate_proj, up_proj, down_proj):
    me = lax.axis_index("sp") % SHARE
    width = gate_proj.shape[1] // SHARE
    gate_up, down = [], []
    for mask in range(SHARE):
        start = (me ^ mask) * width
        piece = jnp.concatenate(
            [
                lax.dynamic_slice_in_dim(gate_proj, start, width, axis=1),
                lax.dynamic_slice_in_dim(up_proj, start, width, axis=1),
            ],
            axis=1,
        )
        gate_up.append(swapped(piece, "sp", mask) if mask else piece)
    for mask in range(SHARE):
        piece = lax.dynamic_slice_in_dim(down_proj, (me ^ mask) * width, width, axis=0)
        down.append(swapped(piece, "sp", mask) if mask else piece)
    return (
        jnp.concatenate(by_place(gate_up, me), axis=0),
        jnp.concatenate(by_place(down, me), axis=1),
    )


def spread(chunk):
    groups = lax.axis_size("sp") // SHARE
    if groups == 4:
        half = chunk.shape[0] // 2
        low = swapped(chunk, "sp", SHARE)
        wrap = swapped(chunk, "sp", 3 * SHARE)
        first = swapped(low[:half], "sp", 3 * SHARE)
        second = swapped(wrap[half:], "sp", SHARE)
        return [chunk, low, jnp.concatenate([first, second], axis=0), wrap]
    chunks = [chunk]
    for bit in bits_of(groups):
        chunks = chunks + [swapped(piece, "sp", SHARE * bit) for piece in chunks]
    return chunks


def gathered(rows, hops):
    for axis, mask in hops:
        rows = jnp.concatenate([rows, swapped(rows, axis, mask)], axis=0)
    return rows


def scattered(partial, hops):
    total = partial
    for axis, mask in reversed(hops):
        half = total.shape[0] // 2
        arrived = swapped(total[half:].astype(jnp.bfloat16), axis, mask)
        total = total[:half].astype(jnp.float32) + arrived.astype(jnp.float32)
    return total


def shards(
    resid,
    queries,
    keys,
    values,
    documents,
    sinks,
    out_proj,
    norm_gain,
    gate_proj,
    up_proj,
    down_proj,
):
    groups = lax.axis_size("sp") // SHARE
    group = lax.axis_index("sp") // SHARE
    gate_up, down = regrouped(gate_proj, up_proj, down_proj)
    gate_up = jnp.concatenate(spread(gate_up), axis=0)
    down = jnp.concatenate(spread(down), axis=1)
    units = down.shape[0]

    attended = attend(queries, keys, values, documents, sinks)
    mid_rows = resid.astype(jnp.float32) + jnp.dot(
        own_rows(attended), out_proj, preferred_element_type=jnp.float32
    )
    normed = norm_rows(mid_rows, norm_gain)
    rows, width = normed.shape
    block = width // groups
    normed = jnp.concatenate(
        [lax.dynamic_slice_in_dim(normed, (group ^ k) * block, block, axis=1) for k in range(groups)],
        axis=1,
    )
    x_hops = [("tp", bit) for bit in bits_of(lax.axis_size("tp"))]
    y_hops = [("sp", 2)]
    core_hops = [("sp", 1)]
    sums = []
    for stream, hops in enumerate((x_hops + y_hops + core_hops, y_hops + x_hops + core_hops)):
        part = normed[stream * rows // 2 : (stream + 1) * rows // 2]
        part = gathered(part, hops)
        acts = jnp.dot(part, gate_up, preferred_element_type=jnp.float32)
        hidden = (jax.nn.silu(acts[:, :units]) * acts[:, units:]).astype(jnp.bfloat16)
        partial = jnp.dot(hidden, down, preferred_element_type=jnp.float32).astype(jnp.bfloat16)
        sums.append(scattered(partial, hops))
    summed = jnp.concatenate(sums, axis=0)
    stack = jnp.stack([summed[:, k * block : (k + 1) * block] for k in range(groups)])
    summed = jnp.concatenate(
        [lax.dynamic_index_in_dim(stack, group ^ k, keepdims=False) for k in range(groups)], axis=1
    )
    return (mid_rows + summed).astype(jnp.bfloat16)


MESH = pl.DeviceIdType.MESH
CHAIN, SIDE, CORES = 4, 2, 2


def fits(mesh):
    return mesh.shape["sp"] == CHAIN * SIDE * CORES and mesh.shape["tp"] == 2


def layer_kernel(
    documents_ref,
    gain_ref,
    sinks_ref,
    resid_hbm,
    queries_hbm,
    keys_hbm,
    values_hbm,
    out_proj_hbm,
    gate_hbm,
    up_hbm,
    down_hbm,
    out_ref,
    q_v,
    k_v,
    v_v,
    halo_docs,
    resid_v,
    out_proj_v,
    att,
    att_out,
    mid,
    tok,
    gu,
    dn,
    acts,
    hid,
    part,
    x_out,
    x_in,
    z_out,
    z_in,
    local_sem,
    halo_s,
    halo_r,
    own_s,
    own_r,
    tok_s,
    tok_r,
    wl,
    wz_s,
    wz_r,
    wy_s,
    wy_r,
    wc_s,
    wc_r,
    rx_s,
    rx_r,
    rz_s,
    rz_r,
):
    sp = lax.axis_index("sp")
    x = lax.axis_index("tp")
    z = sp // (SIDE * CORES)
    y = (sp // CORES) % SIDE
    c = sp % CORES
    hi, lo = z // 2, z % 2
    pair = z + 1 - 2 * lo
    far_mid = 2 - hi
    far_end = 3 - 3 * hi
    is_mid = jnp.where((z == 1) | (z == 2), 1, 0)

    def at(zz, yy, cc, xx):
        return ((zz * SIDE + yy) * CORES + cc, xx)

    to_pair, to_mid, to_end = at(pair, y, c, x), at(far_mid, y, c, x), at(far_end, y, c, x)
    to_y, to_c, to_x = at(z, 1 - y, c, x), at(z, y, 1 - c, x), (sp, 1 - x)
    count = CHAIN * SIDE * CORES
    to_next = (lax.rem(sp + 1, count), x)
    to_prev = (lax.rem(sp + count - 1, count), x)

    rows, own = q_v.shape[0], resid_v.shape[0]
    depth = gate_hbm.shape[0]
    units = gu.shape[2]
    width = mid.shape[1]
    heads = sinks_ref.shape[0]
    kv_heads = k_v.shape[1] // HD
    group = heads // kv_heads
    blocks = rows // WINDOW
    pane = dn.shape[2]
    cols = heads * HD

    def remote(src, dst, send, recv, device):
        return pltpu.make_async_remote_copy(
            src_ref=src, dst_ref=dst, send_sem=send, recv_sem=recv, device_id=device, device_id_type=MESH
        )

    fetch = [
        pltpu.make_async_copy(queries_hbm, q_v, local_sem.at[0]),
        pltpu.make_async_copy(keys_hbm, k_v.at[pl.ds(WINDOW, rows), :], local_sem.at[1]),
        pltpu.make_async_copy(values_hbm, v_v.at[pl.ds(WINDOW, rows), :], local_sem.at[2]),
        pltpu.make_async_copy(resid_hbm, resid_v, local_sem.at[3]),
        pltpu.make_async_copy(out_proj_hbm, out_proj_v, local_sem.at[4]),
    ]
    for copy in fetch:
        copy.start()

    barrier = pltpu.get_barrier_semaphore()
    around = (to_pair, to_mid, to_end, to_y, to_c, to_x, to_next, to_prev)
    for device in around:
        pl.semaphore_signal(barrier, inc=1, device_id=device, device_id_type=MESH)
    pl.semaphore_wait(barrier, len(around))

    last = pl.ds(rows - WINDOW, WINDOW)
    halo = [
        remote(keys_hbm.at[last, :], k_v.at[pl.ds(0, WINDOW), :], halo_s.at[0], halo_r.at[0], to_next),
        remote(values_hbm.at[last, :], v_v.at[pl.ds(0, WINDOW), :], halo_s.at[1], halo_r.at[1], to_next),
        remote(documents_ref.at[pl.ds(blocks - 1, 1), :], halo_docs, halo_s.at[2], halo_r.at[2], to_next),
    ]
    for copy in halo:
        copy.start()

    mid_plane = is_mid == 1
    rows_z = (z, jnp.where(mid_plane, far_end, pair), far_mid, jnp.where(mid_plane, pair, far_end))
    cols_z = (
        z,
        jnp.where(mid_plane, far_mid, far_end),
        jnp.where(mid_plane, pair, far_mid),
        jnp.where(mid_plane, far_end, pair),
    )
    z_of = (rows_z, rows_z, cols_z, rows_z, rows_z, rows_z, rows_z)
    row_slots = (
        jnp.where(mid_plane, 1, 3),
        jnp.where(mid_plane, 2, 1),
        jnp.where(mid_plane, 2, 3),
    )
    col_slots = (
        jnp.where(mid_plane, 3, 2),
        jnp.where(mid_plane, 1, 3),
        jnp.where(mid_plane, 2, 1),
    )
    upper, lower = (0, depth // 2), (depth // 2, depth // 2)
    spans_of = ((0, depth), (0, depth), None, upper, lower, upper, lower)
    array_of = (0, 1, 2, 1, 1, 0, 0)
    late = (5, 6, 3, 4)

    def place(kind, zz, yy, cc):
        if kind == 2:
            return dn.at[zz * SIDE + yy, :, pl.ds(pl.multiple_of(cc * depth, depth), depth)]
        source = (zz * SIDE + yy) * CORES + cc
        first, count = spans_of[kind]
        return gu.at[array_of[kind], pl.ds(pl.multiple_of(source * depth + first, count), count), :]

    def shard(kind, half):
        start = pl.ds(pl.multiple_of(half * units, WINDOW), units)
        if kind == 2:
            return down_hbm.at[start, :]
        return (gate_hbm, up_hbm)[array_of[kind]].at[pl.ds(*spans_of[kind]), start]

    def z_send(kind, dest):
        half, device = ((1 - lo, to_pair), (hi, to_mid), (1 - hi, to_end))[dest]
        slot = (col_slots if kind == 2 else row_slots)[dest]
        return remote(
            shard(kind, half), place(kind, z, y, c), wz_s.at[dest, kind], wz_r.at[slot - 1, kind], device
        )

    def z_arrival(kind, slot):
        where = place(kind, z_of[kind][slot], y, c)
        return remote(where, where, wz_s.at[slot - 1, kind], wz_r.at[slot - 1, kind], to_pair)

    def y_send(kind, slot):
        where = place(kind, z_of[kind][slot], y, c)
        return remote(
            shard(kind, lo) if slot == 0 else where, where, wy_s.at[slot, kind], wy_r.at[slot, kind], to_y
        )

    def y_arrival(kind, slot):
        where = place(kind, z_of[kind][slot], 1 - y, c)
        return remote(where, where, wy_s.at[slot, kind], wy_r.at[slot, kind], to_y)

    def c_send(kind, slot, other):
        where = place(kind, z_of[kind][slot], 1 - y if other else y, c)
        source = shard(kind, lo) if slot == 0 and not other else where
        return remote(source, where, wc_s.at[slot, other, kind], wc_r.at[slot, other, kind], to_c)

    def c_arrival(kind, slot, other):
        where = place(kind, z_of[kind][slot], 1 - y if other else y, 1 - c)
        return remote(where, where, wc_s.at[slot, other, kind], wc_r.at[slot, other, kind], to_c)

    kept = [
        pltpu.make_async_copy(shard(kind, lo), place(kind, z, y, c), wl.at[kind]) for kind in range(3)
    ]

    def z_in_and_on(kind, slot):
        z_arrival(kind, slot).wait_recv()
        y_send(kind, slot).start()
        c_send(kind, slot, 0).start()

    def y_in_and_on(kind, slot):
        y_arrival(kind, slot).wait_recv()
        c_send(kind, slot, 1).start()

    @pl.when(is_mid == 1)
    def _():
        for kind in (0, 1):
            z_send(kind, 0).start()

    @pl.when(is_mid == 0)
    def _():
        for kind in (0, 1):
            z_send(kind, 1).start()

    for kind in (0, 1):
        y_send(kind, 0).start()
        c_send(kind, 0, 0).start()
    c_send(2, 0, 0).start()

    for copy in kept:
        copy.start()

    for copy in fetch[:3]:
        copy.wait()

    row = lax.broadcasted_iota(jnp.int32, (WINDOW, 2 * WINDOW), 0)
    col = lax.broadcasted_iota(jnp.int32, (WINDOW, 2 * WINDOW), 1)
    distance = row + WINDOW - col
    in_window = (distance >= 0) & (distance < WINDOW)

    def attend_block(block, target, target_row, target_col, may_be_first):
        here = documents_ref[pl.ds(block, 1), :]
        back = documents_ref[pl.ds(jnp.maximum(block - 1, 0), 1), :]
        if may_be_first:
            back = jnp.where(block == 0, halo_docs[...], back)
        band = jnp.concatenate([back, here], axis=1).astype(jnp.float32)
        mine = jnp.broadcast_to(here.astype(jnp.float32), (WINDOW, WINDOW)).T
        mine = jnp.concatenate([mine, mine], axis=1)
        visible = in_window & (band == mine)
        if may_be_first:
            visible = visible & (col >= jnp.where((sp == 0) & (block == 0), WINDOW, 0))
        start = pl.multiple_of(block * WINDOW, WINDOW)
        for kv in range(kv_heads):
            k_band = k_v[pl.ds(start, 2 * WINDOW), kv * HD : (kv + 1) * HD]
            v_band = v_v[pl.ds(start, 2 * WINDOW), kv * HD : (kv + 1) * HD]
            pieces = []
            for head in range(kv * group, (kv + 1) * group):
                q = q_v[pl.ds(start, WINDOW), head * HD : (head + 1) * HD]
                scores = lax.dot_general(
                    q, k_band, (((1,), (1,)), ((), ())), preferred_element_type=jnp.float32
                ) * HD ** (-0.5)
                scores = jnp.where(visible, scores, -jnp.inf)
                sink = sinks_ref[head]
                top = jnp.maximum(jnp.max(scores, axis=1, keepdims=True), sink)
                raw = jnp.exp(scores - top)
                total = jnp.sum(raw, axis=1, keepdims=True) + jnp.exp(sink - top)
                weights = (raw / total).astype(jnp.bfloat16)
                pieces.append(jnp.dot(weights, v_band, preferred_element_type=jnp.float32))
            merged = jnp.concatenate(pieces, axis=1).astype(jnp.bfloat16)
            at_col = target_col + kv * group * HD
            if not isinstance(at_col, int):
                at_col = pl.multiple_of(at_col, WINDOW)
            target[pl.ds(target_row, WINDOW), pl.ds(at_col, group * HD)] = merged

    own_blocks = own // WINDOW
    my_cols = pl.ds(pl.multiple_of(x * cols, WINDOW), cols)

    def own_send(part_index):
        part_rows = pl.ds(part_index * WINDOW, WINDOW)
        return remote(
            att_out.at[part_rows, :],
            att.at[part_rows, my_cols],
            own_s.at[part_index],
            own_r.at[part_index],
            to_x,
        )

    for b in reversed(range(own_blocks)):
        if b == 0:
            for copy in halo:
                copy.wait_recv()
        attend_block((1 - x) * own_blocks + b, att_out, b * WINDOW, 0, b == 0)
        own_send(b).start()
        attend_block(x * own_blocks + b, att, b * WINDOW, x * cols, b == 0)

    their_cols = pl.ds(pl.multiple_of((1 - x) * cols, WINDOW), cols)

    for copy in fetch[3:]:
        copy.wait()
    square = jnp.zeros((own, 1), jnp.float32)
    step = 2 * pane
    my_rows = pl.ds(pl.multiple_of(x * cols, WINDOW), cols)
    their_rows = pl.ds(pl.multiple_of((1 - x) * cols, WINDOW), cols)
    for n in range(width // step):
        block_cols = pl.ds(n * step, step)
        mid[:, block_cols] = resid_v[:, block_cols].astype(jnp.float32) + jnp.dot(
            att[:, my_cols], out_proj_v[my_rows, block_cols], preferred_element_type=jnp.float32
        )
    for b in range(own_blocks):
        where = att.at[pl.ds(b * WINDOW, WINDOW), their_cols]
        remote(where, where, own_s.at[b], own_r.at[b], to_x).wait_recv()
    for n in range(width // step):
        block_cols = pl.ds(n * step, step)
        value = mid[:, block_cols] + jnp.dot(
            att[:, their_cols], out_proj_v[their_rows, block_cols], preferred_element_type=jnp.float32
        )
        mid[:, block_cols] = value
        square = square + jnp.sum(value * value, axis=1, keepdims=True)
    scale = lax.rsqrt(square * (1.0 / width) + 1e-06)
    for n in range(width // step):
        block_cols = pl.ds(n * step, step)
        tok[pl.ds(0, own), block_cols] = (
            mid[:, block_cols] * scale * gain_ref[:, block_cols]
        ).astype(jnp.bfloat16)

    bits = own // 2

    def tok_at(slot, bit):
        return tok.at[pl.ds(slot * own + bit * bits, bits), :]

    tok_z = [remote(tok_at(0, i), tok_at(3, i), tok_s.at[0, i], tok_r.at[0, i], to_pair) for i in range(2)]
    tok_x = [remote(tok_at(0, i), tok_at(1, i), tok_s.at[1, i], tok_r.at[1, i], to_x) for i in range(2)]
    tok_on = [remote(tok_at(3, i), tok_at(2, i), tok_s.at[2, i], tok_r.at[2, i], to_x) for i in range(2)]
    for i in range(2):
        tok_z[i].start()
        tok_x[i].start()

    @pl.when(is_mid == 1)
    def _():
        for dest in (2, 1):
            for kind in (0, 1):
                z_send(kind, dest).start()
        z_send(2, 1).start()

    @pl.when(is_mid == 0)
    def _():
        for dest in (0, 2):
            for kind in late:
                z_send(kind, dest).start()
        for dest in (2, 0, 1):
            z_send(2, dest).start()

    def ready(kind, slot):
        c_arrival(kind, slot, 0).wait_recv()
        c_arrival(kind, slot, 1).wait_recv()

    tall = own * 4

    def gate_up(slot, spans, first=False, final=None, kinds=(0, 1)):
        source = z_of[0][slot] * (SIDE * CORES * depth)
        deep = pl.ds(pl.multiple_of(source, SIDE * CORES * depth), SIDE * CORES * depth)

        def tile(start, size):
            at_units = pl.ds(start, size)
            for position, (at_row, height) in enumerate(spans):
                span = pl.ds(at_row, height)
                for kind in kinds:
                    value = jnp.dot(
                        tok[span, deep], gu[kind, deep, at_units], preferred_element_type=jnp.float32
                    )
                    if not first:
                        value = value + acts[kind, span, at_units]
                    if final is None:
                        acts[kind, span, at_units] = value
                if final is not None:
                    gate_acts = acts[0, span, at_units]
                    hid[pl.ds(final + position * height, height), at_units] = (
                        gate_acts / (1.0 + jnp.exp(-gate_acts)) * value
                    ).astype(jnp.bfloat16)

        whole = units // pane

        def body(n, carry):
            tile(pl.multiple_of(n * pane, pane), pane)
            return carry

        lax.fori_loop(0, whole, body, 0)
        if units % pane:
            tile(whole * pane, units % pane)

    def gate_only(slot):
        gate_up(slot, near, kinds=(0,))
        gate_up(slot, far, kinds=(0,))

    def last_up(slot, spans, final):
        gate_up(slot, spans, final=final, kinds=(1,))

    half = tall // 2
    near, theirs, paired = ((0, half),), ((half, own),), ((half + own, own),)
    far = ((half, half),)
    sent, held = ((own, half),), ((0, own), (tall - own, own))

    panes = [(slot, other) for slot in range(4) for other in range(2)]
    pair_first = ()

    def pane_of(i):
        slot, other = panes[i]
        return z_of[2][slot] * SIDE + (1 - y if other else y)

    def x_sum(i):
        j = pane_of(i)
        device = to_pair if i in pair_first else to_x
        return remote(x_out.at[j], x_in.at[j], rx_s.at[i], rx_r.at[i], device)

    def z_sum(i):
        j = pane_of(i)
        device = to_x if i in pair_first else to_pair
        return remote(z_out.at[j], z_in.at[j], rz_s.at[j], rz_r.at[j], device)

    def down_sent(i):
        j = pane_of(i)
        x_out[j] = jnp.dot(
            hid[pl.ds(0, half), :], dn[j], preferred_element_type=jnp.float32
        ).astype(jnp.bfloat16)
        x_sum(i).start()

    def down_held(i):
        j = pane_of(i)
        part[j] = jnp.dot(hid[pl.ds(half, half), :], dn[j], preferred_element_type=jnp.float32)

    def fold(i):
        j = pane_of(i)
        x_sum(i).wait_recv()
        total = part[j] + x_in[j].astype(jnp.float32)
        z_out[j] = total[own:, :].astype(jnp.bfloat16)
        z_sum(i).start()
        part[j, pl.ds(0, own), :] = total[:own, :]

    def finish(i):
        j = pane_of(i)
        z_sum(i).wait_recv()
        at_cols = pl.ds(pl.multiple_of(j * pane, pane), pane)
        out_ref[:, at_cols] = (
            mid[:, at_cols] + (part[j, pl.ds(0, own), :] + z_in[j].astype(jnp.float32))
        ).astype(jnp.bfloat16)

    def tok_forward(i):
        tok_z[i].wait_recv()
        tok_on[i].start()

    def tok_wait(group):
        for copy in group:
            copy.wait_recv()

    def late_down(dest):
        z_send(2, dest).start()

    def own_down():
        y_send(2, 0).start()

    def apart(ends, mids):
        for want, listed in ((0, ends), (1, mids)):

            @pl.when(is_mid == want)
            def _():
                run(listed)

    def kept_wait(kind):
        kept[kind].wait()

    steps = (
        (y_in_and_on, 0, 0),
        (z_in_and_on, 0, 1),
        (y_in_and_on, 1, 0),
        (z_in_and_on, 1, 1),
        (y_in_and_on, 0, 1),
        (
            apart,
            ((z_in_and_on, 0, 2), (y_in_and_on, 1, 1), (z_in_and_on, 1, 2)),
            ((tok_forward, 0), (y_in_and_on, 1, 1), (own_down,), (tok_forward, 1)),
        ),
        (tok_wait, tok_x),
        (kept_wait, 0),
        (kept_wait, 1),
        (ready, 0, 0),
        (ready, 1, 0),
        (gate_up, 0, near, True),
        (ready, 0, 1),
        (ready, 1, 1),
        (gate_up, 1, near),
        (
            apart,
            (
                (y_in_and_on, 0, 2),
                (tok_forward, 0),
                (own_down,),
                (y_in_and_on, 1, 2),
                (tok_forward, 1),
            ),
            ((z_in_and_on, 0, 2), (z_in_and_on, 5, 3), (z_in_and_on, 6, 3), (z_in_and_on, 1, 2)),
        ),
        (gate_up, 0, paired, True),
        (apart, ((z_in_and_on, 5, 3),), ((z_in_and_on, 3, 3), (y_in_and_on, 0, 2))),
        (gate_up, 1, paired),
        (
            apart,
            (
                (ready, 0, 2),
                (ready, 1, 2),
                (gate_up, 2, near),
                (z_in_and_on, 6, 3),
                (gate_up, 2, paired),
                (z_in_and_on, 3, 3),
            ),
            ((z_in_and_on, 4, 3), (y_in_and_on, 5, 3)),
        ),
        (tok_wait, tok_on),
        (gate_up, 0, theirs, True),
        (
            apart,
            ((z_in_and_on, 4, 3), (y_in_and_on, 5, 3), (y_in_and_on, 6, 3)),
            ((y_in_and_on, 6, 3),),
        ),
        (gate_up, 1, theirs),
        (
            apart,
            (),
            (
                (y_in_and_on, 1, 2),
                (ready, 0, 2),
                (ready, 1, 2),
                (gate_up, 2, near),
                (gate_up, 2, paired),
                (late_down, 2),
            ),
        ),
        (gate_up, 2, theirs),
        (y_in_and_on, 2, 0),
        (y_in_and_on, 3, 3),
        (ready, 5, 3),
        (ready, 6, 3),
        (gate_only, 3),
        (y_in_and_on, 4, 3),
        (apart, (), ((late_down, 0),)),
        (z_in_and_on, 2, 1),
        (ready, 3, 3),
        (ready, 4, 3),
        (last_up, 3, sent, 0),
        (kept_wait, 2),
        (ready, 2, 0),
        (down_sent, 0),
        (down_sent, 1),
        (last_up, 3, held, half),
        (down_held, 0),
        (y_in_and_on, 2, 1),
        (z_in_and_on, 2, 2),
        (fold, 0),
        (ready, 2, 1),
        (down_sent, 2),
        (down_sent, 3),
        (down_held, 1),
        (fold, 1),
        (z_in_and_on, 2, 3),
        (y_in_and_on, 2, 2),
        (down_held, 2),
        (ready, 2, 2),
        (down_sent, 4),
        (down_sent, 5),
        (fold, 2),
        (down_held, 3),
        (y_in_and_on, 2, 3),
        (ready, 2, 3),
        (down_sent, 6),
        (down_sent, 7),
        (fold, 3),
        (down_held, 4),
        (fold, 4),
        (down_held, 5),
        (fold, 5),
        (down_held, 6),
        (down_held, 7),
        (fold, 6),
        (fold, 7),
        (finish, 0),
        (finish, 1),
        (finish, 2),
        (finish, 3),
        (finish, 4),
        (finish, 5),
        (finish, 6),
        (finish, 7),
    )

    def run(listed):
        for action, *given in listed:
            if action is apart:
                apart(*given)
                continue
            action(*given)

    run(steps)

    for copy in halo:
        copy.wait_send()
    for b in range(own_blocks):
        own_send(b).wait_send()
    for copy in tok_z + tok_x + tok_on:
        copy.wait_send()
    for kind in (0, 1, 2):
        for slot in range(3):
            y_send(kind, slot).wait_send()
            for other in range(2):
                c_send(kind, slot, other).wait_send()
    for kind in (2,) + late:
        y_send(kind, 3).wait_send()
        for other in range(2):
            c_send(kind, 3, other).wait_send()
    for dest in range(3):
        z_send(2, dest).wait_send()

    @pl.when(is_mid == 1)
    def _():
        for kind in (0, 1):
            for dest in range(3):
                z_send(kind, dest).wait_send()

    @pl.when(is_mid == 0)
    def _():
        for kind in (0, 1):
            z_send(kind, 1).wait_send()
        for kind in late:
            z_send(kind, 0).wait_send()
            z_send(kind, 2).wait_send()

    for i in range(8):
        x_sum(i).wait_send()
        z_sum(i).wait_send()


def one_kernel(
    resid, queries, keys, values, documents, sinks, out_proj, norm_gain, gate_proj, up_proj, down_proj
):
    rows, own, width = queries.shape[0], resid.shape[0], resid.shape[1]
    units = gate_proj.shape[1] // 2
    deep = gate_proj.shape[0] * CHAIN * SIDE * CORES
    pane = gate_proj.shape[0] * CORES
    panes = width // pane
    heads_cols, kv_cols = queries.shape[1], keys.shape[1]
    bf16, f32 = jnp.bfloat16, jnp.float32
    vmem = pl.BlockSpec(memory_space=pltpu.VMEM)
    anywhere = pl.BlockSpec(memory_space=pl.ANY)
    dma = pltpu.SemaphoreType.DMA
    tall = 4 * own
    return pl.pallas_call(
        layer_kernel,
        out_shape=jax.ShapeDtypeStruct((own, width), bf16),
        in_specs=[vmem, vmem, pl.BlockSpec(memory_space=pltpu.SMEM)] + [anywhere] * 8,
        out_specs=vmem,
        scratch_shapes=[
            pltpu.VMEM((rows, heads_cols), bf16),
            pltpu.VMEM((rows + WINDOW, kv_cols), bf16),
            pltpu.VMEM((rows + WINDOW, kv_cols), bf16),
            pltpu.VMEM((1, WINDOW), jnp.int32),
            pltpu.VMEM((own, width), bf16),
            pltpu.VMEM(out_proj.shape, bf16),
            pltpu.VMEM((own, out_proj.shape[0]), bf16),
            pltpu.VMEM((own, heads_cols), bf16),
            pltpu.VMEM((own, width), f32),
            pltpu.VMEM((tall, width), bf16),
            pltpu.VMEM((2, deep, units), bf16),
            pltpu.VMEM((panes, units, pane), bf16),
            pltpu.VMEM((2, tall, units), f32),
            pltpu.VMEM((tall, units), bf16),
            pltpu.VMEM((panes, tall // 2, pane), f32),
            pltpu.VMEM((panes, tall // 2, pane), bf16),
            pltpu.VMEM((panes, tall // 2, pane), bf16),
            pltpu.VMEM((panes, own, pane), bf16),
            pltpu.VMEM((panes, own, pane), bf16),
            dma((5,)),
            dma((3,)),
            dma((3,)),
            dma((own // WINDOW,)),
            dma((own // WINDOW,)),
            dma((3, 2)),
            dma((3, 2)),
            dma((3,)),
            dma((3, 7)),
            dma((3, 7)),
            dma((4, 7)),
            dma((4, 7)),
            dma((4, 2, 7)),
            dma((4, 2, 7)),
            dma((panes,)),
            dma((panes,)),
            dma((panes,)),
            dma((panes,)),
        ],
        compiler_params=pltpu.CompilerParams(
            collective_id=0, has_side_effects=True, vmem_limit_bytes=66_000_000
        ),
        name="layer",
    )(
        documents.reshape(rows // WINDOW, WINDOW),
        norm_gain.reshape(1, width),
        sinks,
        resid,
        queries,
        keys,
        values,
        out_proj,
        gate_proj,
        up_proj,
        down_proj,
    )


def solution(mesh):
    in_specs = (
        P(("sp", "tp"), None),
        P("sp", "tp"),
        P("sp", "tp"),
        P("sp", "tp"),
        P("sp"),
        P("tp"),
        P(),
        P(),
        P("sp", "tp"),
        P("sp", "tp"),
        P("tp", "sp"),
    )
    out_specs = P(("sp", "tp"), None)
    if fits(mesh):
        program = lambda *arrays: one_kernel(*arrays)
        return jax.shard_map(
            program, mesh=mesh, in_specs=in_specs, out_specs=out_specs, check_vma=False
        )
    return jax.shard_map(shards, mesh=mesh, in_specs=in_specs, out_specs=out_specs, check_vma=False)
```

```python
import jax
import jax.numpy as jnp
from jax import lax
from jax.experimental import pallas as pl
from jax.experimental.pallas import tpu as pltpu
from jax.sharding import PartitionSpec as P

HD = 64
WINDOW = 128
SHARE = 4


def passed_along(value, axis, steps):
    count = lax.axis_size(axis)
    first, last = (max(0, -steps), min(count, count - steps))
    return lax.ppermute(value, axis, [(source, source + steps) for source in range(first, last)])


def swapped(value, axis, mask):
    count = lax.axis_size(axis)
    return lax.ppermute(value, axis, [(source, source ^ mask) for source in range(count)])


def bits_of(count):
    return [1 << bit for bit in range(count.bit_length() - 1)]


def attend(queries, keys, values, documents, sinks):
    rows = queries.shape[0]
    kv_heads = keys.shape[1] // HD
    group = queries.shape[1] // HD // kv_heads
    blocks = rows // WINDOW
    key_value = jnp.concatenate([keys, values], axis=1)
    tail_pair, tail_docs = passed_along(
        (key_value[rows - WINDOW :], documents[rows - WINDOW :].astype(jnp.bfloat16)), "sp", 1
    )
    ext_pair = jnp.concatenate([tail_pair, key_value], axis=0).reshape(
        blocks + 1, WINDOW, 2 * kv_heads * HD
    )
    ext_docs = jnp.concatenate([tail_docs.astype(jnp.int32), documents], axis=0).reshape(
        blocks + 1, WINDOW
    )
    band = jnp.concatenate([ext_pair[:-1], ext_pair[1:]], axis=1)
    band_keys = band[:, :, : kv_heads * HD].reshape(blocks, 2 * WINDOW, kv_heads, HD)
    band_values = band[:, :, kv_heads * HD :].reshape(blocks, 2 * WINDOW, kv_heads, HD)
    band_docs = jnp.concatenate([ext_docs[:-1], ext_docs[1:]], axis=1)
    query_docs = documents.reshape(blocks, WINDOW)
    offset = lax.axis_index("sp") * rows
    distance = jnp.arange(WINDOW)[:, None] + WINDOW - jnp.arange(2 * WINDOW)[None, :]
    key_pos = (
        offset + jnp.arange(blocks)[:, None] * WINDOW + jnp.arange(2 * WINDOW)[None, :] - WINDOW
    )
    visible = (
        ((distance >= 0) & (distance < WINDOW))[None]
        & (key_pos >= 0)[:, None, :]
        & (band_docs[:, None, :] == query_docs[:, :, None])
    )
    query_blocks = queries.reshape(blocks, WINDOW, kv_heads, group, HD)
    scores = jnp.einsum(
        "nikgd,njkd->nkgij", query_blocks, band_keys, preferred_element_type=jnp.float32
    ) * HD ** (-0.5)
    scores = jnp.where(visible[:, None, None], scores, -jnp.inf)
    sink_logit = sinks.reshape(kv_heads, group)[None, :, :, None, None]
    row_top = jnp.maximum(jnp.max(scores, axis=-1, keepdims=True), sink_logit)
    raw_weights = jnp.exp(scores - row_top)
    totals = jnp.sum(raw_weights, axis=-1, keepdims=True) + jnp.exp(sink_logit - row_top)
    weights = (raw_weights / totals).astype(jnp.bfloat16)
    attended = jnp.einsum(
        "nkgij,njkd->nikgd", weights, band_values, preferred_element_type=jnp.float32
    )
    return attended.astype(jnp.bfloat16).reshape(rows, kv_heads * group * HD)


def norm_rows(mid_rows, norm_gain):
    scale = lax.rsqrt(jnp.mean(mid_rows * mid_rows, axis=-1, keepdims=True) + 1e-06)
    return (mid_rows * scale * norm_gain).astype(jnp.bfloat16)


def by_place(pieces, me):
    for bit in bits_of(len(pieces)):
        flip = (me & bit) != 0
        pieces = [jnp.where(flip, pieces[r ^ bit], pieces[r]) for r in range(len(pieces))]
    return pieces


def own_rows(attended):
    count = lax.axis_size("tp")
    me = lax.axis_index("tp")
    rows = attended.shape[0] // count
    pieces = []
    for mask in range(count):
        piece = lax.dynamic_slice_in_dim(attended, (me ^ mask) * rows, rows)
        pieces.append(swapped(piece, "tp", mask) if mask else piece)
    return jnp.concatenate(by_place(pieces, me), axis=1)


def regrouped(gate_proj, up_proj, down_proj):
    me = lax.axis_index("sp") % SHARE
    width = gate_proj.shape[1] // SHARE
    gate_up, down = [], []
    for mask in range(SHARE):
        start = (me ^ mask) * width
        piece = jnp.concatenate(
            [
                lax.dynamic_slice_in_dim(gate_proj, start, width, axis=1),
                lax.dynamic_slice_in_dim(up_proj, start, width, axis=1),
            ],
            axis=1,
        )
        gate_up.append(swapped(piece, "sp", mask) if mask else piece)
    for mask in range(SHARE):
        piece = lax.dynamic_slice_in_dim(down_proj, (me ^ mask) * width, width, axis=0)
        down.append(swapped(piece, "sp", mask) if mask else piece)
    return (
        jnp.concatenate(by_place(gate_up, me), axis=0),
        jnp.concatenate(by_place(down, me), axis=1),
    )


def spread(chunk):
    groups = lax.axis_size("sp") // SHARE
    if groups == 4:
        half = chunk.shape[0] // 2
        low = swapped(chunk, "sp", SHARE)
        wrap = swapped(chunk, "sp", 3 * SHARE)
        first = swapped(low[:half], "sp", 3 * SHARE)
        second = swapped(wrap[half:], "sp", SHARE)
        return [chunk, low, jnp.concatenate([first, second], axis=0), wrap]
    chunks = [chunk]
    for bit in bits_of(groups):
        chunks = chunks + [swapped(piece, "sp", SHARE * bit) for piece in chunks]
    return chunks


def gathered(rows, hops):
    for axis, mask in hops:
        rows = jnp.concatenate([rows, swapped(rows, axis, mask)], axis=0)
    return rows


def scattered(partial, hops):
    total = partial
    for axis, mask in reversed(hops):
        half = total.shape[0] // 2
        arrived = swapped(total[half:].astype(jnp.bfloat16), axis, mask)
        total = total[:half].astype(jnp.float32) + arrived.astype(jnp.float32)
    return total


def shards(
    resid,
    queries,
    keys,
    values,
    documents,
    sinks,
    out_proj,
    norm_gain,
    gate_proj,
    up_proj,
    down_proj,
):
    groups = lax.axis_size("sp") // SHARE
    group = lax.axis_index("sp") // SHARE
    gate_up, down = regrouped(gate_proj, up_proj, down_proj)
    gate_up = jnp.concatenate(spread(gate_up), axis=0)
    down = jnp.concatenate(spread(down), axis=1)
    units = down.shape[0]

    attended = attend(queries, keys, values, documents, sinks)
    mid_rows = resid.astype(jnp.float32) + jnp.dot(
        own_rows(attended), out_proj, preferred_element_type=jnp.float32
    )
    normed = norm_rows(mid_rows, norm_gain)
    rows, width = normed.shape
    block = width // groups
    normed = jnp.concatenate(
        [lax.dynamic_slice_in_dim(normed, (group ^ k) * block, block, axis=1) for k in range(groups)],
        axis=1,
    )
    x_hops = [("tp", bit) for bit in bits_of(lax.axis_size("tp"))]
    y_hops = [("sp", 2)]
    core_hops = [("sp", 1)]
    sums = []
    for stream, hops in enumerate((x_hops + y_hops + core_hops, y_hops + x_hops + core_hops)):
        part = normed[stream * rows // 2 : (stream + 1) * rows // 2]
        part = gathered(part, hops)
        acts = jnp.dot(part, gate_up, preferred_element_type=jnp.float32)
        hidden = (jax.nn.silu(acts[:, :units]) * acts[:, units:]).astype(jnp.bfloat16)
        partial = jnp.dot(hidden, down, preferred_element_type=jnp.float32).astype(jnp.bfloat16)
        sums.append(scattered(partial, hops))
    summed = jnp.concatenate(sums, axis=0)
    stack = jnp.stack([summed[:, k * block : (k + 1) * block] for k in range(groups)])
    summed = jnp.concatenate(
        [lax.dynamic_index_in_dim(stack, group ^ k, keepdims=False) for k in range(groups)], axis=1
    )
    return (mid_rows + summed).astype(jnp.bfloat16)


MESH = pl.DeviceIdType.MESH
CHAIN, SIDE, CORES = 4, 2, 2


def fits(mesh):
    return mesh.shape["sp"] == CHAIN * SIDE * CORES and mesh.shape["tp"] == 2


def layer_kernel(
    documents_ref,
    gain_ref,
    sinks_ref,
    resid_hbm,
    queries_hbm,
    keys_hbm,
    values_hbm,
    out_proj_hbm,
    gate_hbm,
    up_hbm,
    down_hbm,
    out_ref,
    out_v,
    q_v,
    k_v,
    v_v,
    halo_docs,
    resid_v,
    out_proj_v,
    att,
    att_out,
    mid,
    tok,
    gu,
    dn,
    acts,
    hid,
    part,
    x_out,
    x_in,
    z_out,
    z_in,
    local_sem,
    halo_s,
    halo_r,
    own_s,
    own_r,
    tok_s,
    tok_r,
    wl,
    wz_s,
    wz_r,
    wy_s,
    wy_r,
    wc_s,
    wc_r,
    rx_s,
    rx_r,
    rz_s,
    rz_r,
    out_sem,
):
    sp = lax.axis_index("sp")
    x = lax.axis_index("tp")
    z = sp // (SIDE * CORES)
    y = (sp // CORES) % SIDE
    c = sp % CORES
    hi, lo = z // 2, z % 2
    pair = z + 1 - 2 * lo
    far_mid = 2 - hi
    far_end = 3 - 3 * hi
    is_mid = jnp.where((z == 1) | (z == 2), 1, 0)

    def at(zz, yy, cc, xx):
        return ((zz * SIDE + yy) * CORES + cc, xx)

    to_pair, to_mid, to_end = at(pair, y, c, x), at(far_mid, y, c, x), at(far_end, y, c, x)
    to_y, to_c, to_x = at(z, 1 - y, c, x), at(z, y, 1 - c, x), (sp, 1 - x)
    count = CHAIN * SIDE * CORES
    to_next = (lax.rem(sp + 1, count), x)
    to_prev = (lax.rem(sp + count - 1, count), x)

    rows, own = q_v.shape[0], resid_v.shape[0]
    depth = gate_hbm.shape[0]
    units = gu.shape[2]
    width = mid.shape[1]
    heads = sinks_ref.shape[0]
    kv_heads = k_v.shape[1] // HD
    group = heads // kv_heads
    blocks = rows // WINDOW
    pane = dn.shape[2]
    cols = heads * HD

    def remote(src, dst, send, recv, device):
        return pltpu.make_async_remote_copy(
            src_ref=src, dst_ref=dst, send_sem=send, recv_sem=recv, device_id=device, device_id_type=MESH
        )

    fetch = [
        pltpu.make_async_copy(queries_hbm, q_v, local_sem.at[0]),
        pltpu.make_async_copy(keys_hbm, k_v.at[pl.ds(WINDOW, rows), :], local_sem.at[1]),
        pltpu.make_async_copy(values_hbm, v_v.at[pl.ds(WINDOW, rows), :], local_sem.at[2]),
        pltpu.make_async_copy(resid_hbm, resid_v, local_sem.at[3]),
        pltpu.make_async_copy(out_proj_hbm, out_proj_v, local_sem.at[4]),
    ]
    for copy in fetch:
        copy.start()

    barrier = pltpu.get_barrier_semaphore()
    around = (to_pair, to_mid, to_end, to_y, to_c, to_x, to_next, to_prev)
    for device in around:
        pl.semaphore_signal(barrier, inc=1, device_id=device, device_id_type=MESH)
    pl.semaphore_wait(barrier, len(around))

    last = pl.ds(rows - WINDOW, WINDOW)
    halo = [
        remote(keys_hbm.at[last, :], k_v.at[pl.ds(0, WINDOW), :], halo_s.at[0], halo_r.at[0], to_next),
        remote(values_hbm.at[last, :], v_v.at[pl.ds(0, WINDOW), :], halo_s.at[1], halo_r.at[1], to_next),
        remote(documents_ref.at[pl.ds(blocks - 1, 1), :], halo_docs, halo_s.at[2], halo_r.at[2], to_next),
    ]
    for copy in halo:
        copy.start()

    mid_plane = is_mid == 1
    rows_z = (z, jnp.where(mid_plane, far_end, pair), far_mid, jnp.where(mid_plane, pair, far_end))
    cols_z = (z, far_mid, pair, far_end)
    z_of = (rows_z, rows_z, cols_z, rows_z, rows_z, rows_z, rows_z)
    row_slots = (
        jnp.where(mid_plane, 1, 3),
        jnp.where(mid_plane, 2, 1),
        jnp.where(mid_plane, 2, 3),
    )
    col_slots = (2, jnp.where(mid_plane, 1, 3), jnp.where(mid_plane, 1, 3))
    upper, lower = (0, depth // 2), (depth // 2, depth // 2)
    spans_of = ((0, depth), (0, depth), None, upper, lower, upper, lower)
    array_of = (0, 1, 2, 1, 1, 0, 0)
    late = (5, 6, 3, 4)

    def place(kind, zz, yy, cc):
        if kind == 2:
            return dn.at[zz * SIDE + yy, :, pl.ds(pl.multiple_of(cc * depth, depth), depth)]
        source = (zz * SIDE + yy) * CORES + cc
        first, count = spans_of[kind]
        return gu.at[array_of[kind], pl.ds(pl.multiple_of(source * depth + first, count), count), :]

    def shard(kind, half):
        start = pl.ds(pl.multiple_of(half * units, WINDOW), units)
        if kind == 2:
            return down_hbm.at[start, :]
        return (gate_hbm, up_hbm)[array_of[kind]].at[pl.ds(*spans_of[kind]), start]

    def z_send(kind, dest):
        half, device = ((1 - lo, to_pair), (hi, to_mid), (1 - hi, to_end))[dest]
        slot = (col_slots if kind == 2 else row_slots)[dest]
        return remote(
            shard(kind, half), place(kind, z, y, c), wz_s.at[dest, kind], wz_r.at[slot - 1, kind], device
        )

    def z_arrival(kind, slot):
        where = place(kind, z_of[kind][slot], y, c)
        return remote(where, where, wz_s.at[slot - 1, kind], wz_r.at[slot - 1, kind], to_pair)

    def y_send(kind, slot):
        where = place(kind, z_of[kind][slot], y, c)
        return remote(
            shard(kind, lo) if slot == 0 else where, where, wy_s.at[slot, kind], wy_r.at[slot, kind], to_y
        )

    def y_arrival(kind, slot):
        where = place(kind, z_of[kind][slot], 1 - y, c)
        return remote(where, where, wy_s.at[slot, kind], wy_r.at[slot, kind], to_y)

    def c_send(kind, slot, other):
        where = place(kind, z_of[kind][slot], 1 - y if other else y, c)
        source = shard(kind, lo) if slot == 0 and not other else where
        return remote(source, where, wc_s.at[slot, other, kind], wc_r.at[slot, other, kind], to_c)

    def c_arrival(kind, slot, other):
        where = place(kind, z_of[kind][slot], 1 - y if other else y, 1 - c)
        return remote(where, where, wc_s.at[slot, other, kind], wc_r.at[slot, other, kind], to_c)

    kept = [
        pltpu.make_async_copy(shard(kind, lo), place(kind, z, y, c), wl.at[kind]) for kind in range(3)
    ]

    def z_in_and_on(kind, slot):
        z_arrival(kind, slot).wait_recv()
        y_send(kind, slot).start()
        c_send(kind, slot, 0).start()

    def y_in_and_on(kind, slot):
        y_arrival(kind, slot).wait_recv()
        c_send(kind, slot, 1).start()

    @pl.when(is_mid == 1)
    def _():
        for kind in (0, 1):
            z_send(kind, 0).start()

    @pl.when(is_mid == 0)
    def _():
        for kind in (0, 1):
            z_send(kind, 1).start()

    for kind in (0, 1):
        y_send(kind, 0).start()
        c_send(kind, 0, 0).start()
    c_send(2, 0, 0).start()

    for copy in kept:
        copy.start()

    for copy in fetch[:3]:
        copy.wait()

    row = lax.broadcasted_iota(jnp.int32, (WINDOW, 2 * WINDOW), 0)
    col = lax.broadcasted_iota(jnp.int32, (WINDOW, 2 * WINDOW), 1)
    distance = row + WINDOW - col
    in_window = (distance >= 0) & (distance < WINDOW)

    def attend_block(block, target, target_row, target_col, may_be_first):
        here = documents_ref[pl.ds(block, 1), :]
        back = documents_ref[pl.ds(jnp.maximum(block - 1, 0), 1), :]
        if may_be_first:
            back = jnp.where(block == 0, halo_docs[...], back)
        band = jnp.concatenate([back, here], axis=1).astype(jnp.float32)
        mine = jnp.broadcast_to(here.astype(jnp.float32), (WINDOW, WINDOW)).T
        mine = jnp.concatenate([mine, mine], axis=1)
        visible = in_window & (band == mine)
        if may_be_first:
            visible = visible & (col >= jnp.where((sp == 0) & (block == 0), WINDOW, 0))
        start = pl.multiple_of(block * WINDOW, WINDOW)
        for kv in range(kv_heads):
            k_band = k_v[pl.ds(start, 2 * WINDOW), kv * HD : (kv + 1) * HD]
            v_band = v_v[pl.ds(start, 2 * WINDOW), kv * HD : (kv + 1) * HD]
            pieces = []
            for head in range(kv * group, (kv + 1) * group):
                q = q_v[pl.ds(start, WINDOW), head * HD : (head + 1) * HD]
                scores = lax.dot_general(
                    q, k_band, (((1,), (1,)), ((), ())), preferred_element_type=jnp.float32
                ) * HD ** (-0.5)
                scores = jnp.where(visible, scores, -jnp.inf)
                sink = sinks_ref[head]
                top = jnp.maximum(jnp.max(scores, axis=1, keepdims=True), sink)
                raw = jnp.exp(scores - top)
                total = jnp.sum(raw, axis=1, keepdims=True) + jnp.exp(sink - top)
                weights = (raw / total).astype(jnp.bfloat16)
                pieces.append(jnp.dot(weights, v_band, preferred_element_type=jnp.float32))
            merged = jnp.concatenate(pieces, axis=1).astype(jnp.bfloat16)
            at_col = target_col + kv * group * HD
            if not isinstance(at_col, int):
                at_col = pl.multiple_of(at_col, WINDOW)
            target[pl.ds(target_row, WINDOW), pl.ds(at_col, group * HD)] = merged

    own_blocks = own // WINDOW
    my_cols = pl.ds(pl.multiple_of(x * cols, WINDOW), cols)

    def own_send(part_index):
        part_rows = pl.ds(part_index * WINDOW, WINDOW)
        return remote(
            att_out.at[part_rows, :],
            att.at[part_rows, my_cols],
            own_s.at[part_index],
            own_r.at[part_index],
            to_x,
        )

    for b in reversed(range(own_blocks)):
        if b == 0:
            for copy in halo:
                copy.wait_recv()
        attend_block((1 - x) * own_blocks + b, att_out, b * WINDOW, 0, b == 0)
        own_send(b).start()
        attend_block(x * own_blocks + b, att, b * WINDOW, x * cols, b == 0)

    their_cols = pl.ds(pl.multiple_of((1 - x) * cols, WINDOW), cols)

    for copy in fetch[3:]:
        copy.wait()
    square = jnp.zeros((own, 1), jnp.float32)
    step = 2 * pane
    my_rows = pl.ds(pl.multiple_of(x * cols, WINDOW), cols)
    their_rows = pl.ds(pl.multiple_of((1 - x) * cols, WINDOW), cols)
    for n in range(width // step):
        block_cols = pl.ds(n * step, step)
        mid[:, block_cols] = resid_v[:, block_cols].astype(jnp.float32) + jnp.dot(
            att[:, my_cols], out_proj_v[my_rows, block_cols], preferred_element_type=jnp.float32
        )
    for b in range(own_blocks):
        where = att.at[pl.ds(b * WINDOW, WINDOW), their_cols]
        remote(where, where, own_s.at[b], own_r.at[b], to_x).wait_recv()
    for n in range(width // step):
        block_cols = pl.ds(n * step, step)
        value = mid[:, block_cols] + jnp.dot(
            att[:, their_cols], out_proj_v[their_rows, block_cols], preferred_element_type=jnp.float32
        )
        mid[:, block_cols] = value
        square = square + jnp.sum(value * value, axis=1, keepdims=True)
    scale = lax.rsqrt(square * (1.0 / width) + 1e-06)
    for n in range(width // step):
        block_cols = pl.ds(n * step, step)
        tok[pl.ds(0, own), block_cols] = (
            mid[:, block_cols] * scale * gain_ref[:, block_cols]
        ).astype(jnp.bfloat16)

    bits = own // 2

    def tok_at(slot, bit):
        return tok.at[pl.ds(slot * own + bit * bits, bits), :]

    tok_z = [remote(tok_at(0, i), tok_at(3, i), tok_s.at[0, i], tok_r.at[0, i], to_pair) for i in range(2)]
    tok_x = [remote(tok_at(0, i), tok_at(1, i), tok_s.at[1, i], tok_r.at[1, i], to_x) for i in range(2)]
    tok_on = [remote(tok_at(3, i), tok_at(2, i), tok_s.at[2, i], tok_r.at[2, i], to_x) for i in range(2)]
    for i in range(2):
        tok_z[i].start()
        tok_x[i].start()

    @pl.when(is_mid == 1)
    def _():
        for dest in (2, 1):
            for kind in (0, 1):
                z_send(kind, dest).start()
        z_send(2, 1).start()

    @pl.when(is_mid == 0)
    def _():
        for dest in (0, 2):
            for kind in late:
                z_send(kind, dest).start()
        z_send(2, 0).start()

    def ready(kind, slot):
        c_arrival(kind, slot, 0).wait_recv()
        c_arrival(kind, slot, 1).wait_recv()

    tall = own * 4

    def gate_up(slot, spans, first=False, final=None, kinds=(0, 1)):
        source = z_of[0][slot] * (SIDE * CORES * depth)
        deep = pl.ds(pl.multiple_of(source, SIDE * CORES * depth), SIDE * CORES * depth)

        def tile(start, size):
            at_units = pl.ds(start, size)
            for position, (at_row, height) in enumerate(spans):
                span = pl.ds(at_row, height)
                for kind in kinds:
                    value = jnp.dot(
                        tok[span, deep], gu[kind, deep, at_units], preferred_element_type=jnp.float32
                    )
                    if not first:
                        value = value + acts[kind, span, at_units]
                    if final is None:
                        acts[kind, span, at_units] = value
                if final is not None:
                    gate_acts = acts[0, span, at_units]
                    hid[pl.ds(final + position * height, height), at_units] = (
                        gate_acts / (1.0 + jnp.exp(-gate_acts)) * value
                    ).astype(jnp.bfloat16)

        whole = units // pane

        def body(n, carry):
            tile(pl.multiple_of(n * pane, pane), pane)
            return carry

        lax.fori_loop(0, whole, body, 0)
        if units % pane:
            tile(whole * pane, units % pane)

    def gate_only(slot):
        gate_up(slot, near, kinds=(0,))
        gate_up(slot, far, kinds=(0,))

    def last_up(slot, spans, final):
        gate_up(slot, spans, final=final, kinds=(1,))

    half = tall // 2
    near, theirs, paired = ((0, half),), ((half, own),), ((half + own, own),)
    far = ((half, half),)
    sent, held = ((own, half),), ((0, own), (tall - own, own))

    panes = [(slot, other) for slot in range(4) for other in range(2)]
    pair_first = ()

    def pane_of(i):
        slot, other = panes[i]
        return z_of[2][slot] * SIDE + (1 - y if other else y)

    whole_rows = {0: pl.ds(0, own), 1: pl.ds(own, own)}

    def first_hop(i, relayed):
        j = pane_of(i)
        device = to_pair if i in pair_first else to_x
        taken = whole_rows[relayed]
        return remote(
            x_out.at[j, taken, :], x_in.at[j, taken, :], rx_s.at[i, relayed], rx_r.at[i, relayed], device
        )

    def second_hop(i):
        j = pane_of(i)
        device = to_x if i in pair_first else to_pair
        return remote(z_out.at[j], z_in.at[j], rz_s.at[j], rz_r.at[j], device)

    def down_sent(i):
        j = pane_of(i)
        x_out[j] = jnp.dot(
            hid[pl.ds(0, half), :], dn[j], preferred_element_type=jnp.float32
        ).astype(jnp.bfloat16)
        first_hop(i, 1).start()

    def down_held(i):
        j = pane_of(i)
        part[j] = jnp.dot(hid[pl.ds(half, half), :], dn[j], preferred_element_type=jnp.float32)

    def send_rest(*given):
        for i in given:
            first_hop(i, 0).start()

    def relay(i):
        j = pane_of(i)
        first_hop(i, 1).wait_recv()
        z_out[j] = (part[j, whole_rows[1], :] + x_in[j, whole_rows[1], :].astype(jnp.float32)).astype(
            jnp.bfloat16
        )
        second_hop(i).start()

    def store(i):
        at_cols = pl.ds(pl.multiple_of(pane_of(i) * pane, pane), pane)
        return pltpu.make_async_copy(out_v.at[:, at_cols], out_ref.at[:, at_cols], out_sem.at[i])

    def finish(i):
        j = pane_of(i)
        first_hop(i, 0).wait_recv()
        second_hop(i).wait_recv()
        at_cols = pl.ds(pl.multiple_of(j * pane, pane), pane)
        summed = part[j, whole_rows[0], :] + x_in[j, whole_rows[0], :].astype(jnp.float32)
        out_v[:, at_cols] = (mid[:, at_cols] + (summed + z_in[j].astype(jnp.float32))).astype(
            jnp.bfloat16
        )
        store(i).start()

    def tok_forward(i):
        tok_z[i].wait_recv()
        tok_on[i].start()

    def tok_wait(group):
        for copy in group:
            copy.wait_recv()

    def late_down(dest):
        z_send(2, dest).start()

    def own_down():
        y_send(2, 0).start()

    def apart(ends, mids):
        for want, listed in ((0, ends), (1, mids)):

            @pl.when(is_mid == want)
            def _():
                run(listed)

    def kept_wait(kind):
        kept[kind].wait()

    def settle():
        for copy in halo:
            copy.wait_send()
        for b in range(own_blocks):
            own_send(b).wait_send()
        for copy in tok_z + tok_x + tok_on:
            copy.wait_send()
        for kind in (0, 1, 2):
            for slot in range(3):
                y_send(kind, slot).wait_send()
                for other in range(2):
                    c_send(kind, slot, other).wait_send()
        for kind in (2,) + late:
            y_send(kind, 3).wait_send()
            for other in range(2):
                c_send(kind, 3, other).wait_send()
        for dest in range(3):
            z_send(2, dest).wait_send()

        @pl.when(is_mid == 1)
        def _():
            for kind in (0, 1):
                for dest in range(3):
                    z_send(kind, dest).wait_send()

        @pl.when(is_mid == 0)
        def _():
            for kind in (0, 1):
                z_send(kind, 1).wait_send()
            for kind in late:
                z_send(kind, 0).wait_send()
                z_send(kind, 2).wait_send()

    steps = (
        (y_in_and_on, 0, 0),
        (z_in_and_on, 0, 1),
        (y_in_and_on, 1, 0),
        (z_in_and_on, 1, 1),
        (y_in_and_on, 0, 1),
        (
            apart,
            ((z_in_and_on, 0, 2), (y_in_and_on, 1, 1), (z_in_and_on, 1, 2)),
            ((tok_forward, 0), (y_in_and_on, 1, 1), (own_down,), (tok_forward, 1)),
        ),
        (tok_wait, tok_x),
        (kept_wait, 0),
        (kept_wait, 1),
        (ready, 0, 0),
        (ready, 1, 0),
        (gate_up, 0, near, True),
        (ready, 0, 1),
        (ready, 1, 1),
        (gate_up, 1, near),
        (
            apart,
            (
                (y_in_and_on, 0, 2),
                (tok_forward, 0),
                (own_down,),
                (y_in_and_on, 1, 2),
                (tok_forward, 1),
            ),
            ((z_in_and_on, 0, 2), (z_in_and_on, 5, 3), (z_in_and_on, 6, 3), (z_in_and_on, 1, 2)),
        ),
        (gate_up, 0, paired, True),
        (apart, ((z_in_and_on, 5, 3),), ((z_in_and_on, 3, 3), (y_in_and_on, 0, 2))),
        (gate_up, 1, paired),
        (
            apart,
            (
                (ready, 0, 2),
                (ready, 1, 2),
                (gate_up, 2, near),
                (z_in_and_on, 6, 3),
                (gate_up, 2, paired),
                (z_in_and_on, 3, 3),
            ),
            ((z_in_and_on, 4, 3), (y_in_and_on, 5, 3)),
        ),
        (tok_wait, tok_on),
        (gate_up, 0, theirs, True),
        (apart, (), ((y_in_and_on, 6, 3),)),
        (gate_up, 1, theirs),
        (
            apart,
            (
                (z_in_and_on, 4, 3),
                (y_in_and_on, 5, 3),
                (y_in_and_on, 6, 3),
                (gate_up, 2, theirs),
                (ready, 5, 3),
                (ready, 6, 3),
                (gate_only, 3),
            ),
            (
                (late_down, 2),
                (ready, 5, 3),
                (ready, 6, 3),
                (gate_only, 3),
                (y_in_and_on, 1, 2),
                (y_in_and_on, 2, 0),
                (late_down, 0),
                (ready, 0, 2),
                (ready, 1, 2),
                (gate_up, 2, near),
                (y_in_and_on, 3, 3),
                (gate_up, 2, far),
            ),
        ),
        (apart, ((y_in_and_on, 2, 0), (y_in_and_on, 3, 3)), ()),
        (y_in_and_on, 4, 3),
        (ready, 3, 3),
        (ready, 4, 3),
        (last_up, 3, sent, 0),
        (kept_wait, 2),
        (ready, 2, 0),
        (down_sent, 0),
        (apart, ((late_down, 1), (late_down, 2)), ()),
        (z_in_and_on, 2, 1),
        (send_rest, 0),
        (down_sent, 1),
        (send_rest, 1),
        (last_up, 3, held, half),
        (z_in_and_on, 2, 2),
        (down_held, 0),
        (y_in_and_on, 2, 1),
        (down_held, 1),
        (ready, 2, 1),
        (down_sent, 2),
        (send_rest, 2),
        (apart, (), ((z_in_and_on, 2, 3),)),
        (down_sent, 3),
        (send_rest, 3),
        (relay, 0),
        (relay, 1),
        (y_in_and_on, 2, 2),
        (down_held, 2),
        (ready, 2, 2),
        (down_sent, 4),
        (send_rest, 4),
        (down_sent, 5),
        (send_rest, 5),
        (apart, ((z_in_and_on, 2, 3),), ()),
        (down_held, 3),
        (relay, 2),
        (relay, 3),
        (y_in_and_on, 2, 3),
        (ready, 2, 3),
        (down_sent, 6),
        (down_sent, 7),
        (send_rest, 6, 7),
        (down_held, 4),
        (relay, 4),
        (down_held, 5),
        (down_held, 6),
        (relay, 5),
        (down_held, 7),
        (settle,),
        (relay, 6),
        (relay, 7),
        (finish, 0),
        (finish, 1),
        (finish, 2),
        (finish, 3),
        (finish, 4),
        (finish, 5),
        (finish, 6),
        (finish, 7),
    )

    def run(listed):
        for action, *given in listed:
            if action is apart:
                apart(*given)
                continue
            action(*given)

    run(steps)

    for i in range(len(panes)):
        first_hop(i, 0).wait_send()
        first_hop(i, 1).wait_send()
        second_hop(i).wait_send()
    for i in range(len(panes)):
        store(i).wait()


def one_kernel(
    resid, queries, keys, values, documents, sinks, out_proj, norm_gain, gate_proj, up_proj, down_proj
):
    rows, own, width = queries.shape[0], resid.shape[0], resid.shape[1]
    units = gate_proj.shape[1] // 2
    deep = gate_proj.shape[0] * CHAIN * SIDE * CORES
    pane = gate_proj.shape[0] * CORES
    panes = width // pane
    heads_cols, kv_cols = queries.shape[1], keys.shape[1]
    bf16, f32 = jnp.bfloat16, jnp.float32
    vmem = pl.BlockSpec(memory_space=pltpu.VMEM)
    anywhere = pl.BlockSpec(memory_space=pl.ANY)
    dma = pltpu.SemaphoreType.DMA
    tall = 4 * own
    return pl.pallas_call(
        layer_kernel,
        out_shape=jax.ShapeDtypeStruct((own, width), bf16),
        in_specs=[vmem, vmem, pl.BlockSpec(memory_space=pltpu.SMEM)] + [anywhere] * 8,
        out_specs=anywhere,
        scratch_shapes=[
            pltpu.VMEM((own, width), bf16),
            pltpu.VMEM((rows, heads_cols), bf16),
            pltpu.VMEM((rows + WINDOW, kv_cols), bf16),
            pltpu.VMEM((rows + WINDOW, kv_cols), bf16),
            pltpu.VMEM((1, WINDOW), jnp.int32),
            pltpu.VMEM((own, width), bf16),
            pltpu.VMEM(out_proj.shape, bf16),
            pltpu.VMEM((own, out_proj.shape[0]), bf16),
            pltpu.VMEM((own, heads_cols), bf16),
            pltpu.VMEM((own, width), f32),
            pltpu.VMEM((tall, width), bf16),
            pltpu.VMEM((2, deep, units), bf16),
            pltpu.VMEM((panes, units, pane), bf16),
            pltpu.VMEM((2, tall, units), f32),
            pltpu.VMEM((tall, units), bf16),
            pltpu.VMEM((panes, tall // 2, pane), f32),
            pltpu.VMEM((panes, tall // 2, pane), bf16),
            pltpu.VMEM((panes, tall // 2, pane), bf16),
            pltpu.VMEM((panes, own, pane), bf16),
            pltpu.VMEM((panes, own, pane), bf16),
            dma((5,)),
            dma((3,)),
            dma((3,)),
            dma((own // WINDOW,)),
            dma((own // WINDOW,)),
            dma((3, 2)),
            dma((3, 2)),
            dma((3,)),
            dma((3, 7)),
            dma((3, 7)),
            dma((4, 7)),
            dma((4, 7)),
            dma((4, 2, 7)),
            dma((4, 2, 7)),
            dma((panes, 2)),
            dma((panes, 2)),
            dma((panes,)),
            dma((panes,)),
            dma((panes,)),
        ],
        compiler_params=pltpu.CompilerParams(
            collective_id=0, has_side_effects=True, vmem_limit_bytes=66_000_000
        ),
        name="layer",
    )(
        documents.reshape(rows // WINDOW, WINDOW),
        norm_gain.reshape(1, width),
        sinks,
        resid,
        queries,
        keys,
        values,
        out_proj,
        gate_proj,
        up_proj,
        down_proj,
    )


def solution(mesh):
    in_specs = (
        P(("sp", "tp"), None),
        P("sp", "tp"),
        P("sp", "tp"),
        P("sp", "tp"),
        P("sp"),
        P("tp"),
        P(),
        P(),
        P("sp", "tp"),
        P("sp", "tp"),
        P("tp", "sp"),
    )
    out_specs = P(("sp", "tp"), None)
    if fits(mesh):
        program = lambda *arrays: one_kernel(*arrays)
        return jax.shard_map(
            program, mesh=mesh, in_specs=in_specs, out_specs=out_specs, check_vma=False
        )
    return jax.shard_map(shards, mesh=mesh, in_specs=in_specs, out_specs=out_specs, check_vma=False)
```

```python
import jax
import jax.numpy as jnp
from jax import lax
from jax.experimental import pallas as pl
from jax.experimental.pallas import tpu as pltpu
from jax.sharding import PartitionSpec as P

HD = 64
WINDOW = 128
SHARE = 4


def passed_along(value, axis, steps):
    count = lax.axis_size(axis)
    first, last = (max(0, -steps), min(count, count - steps))
    return lax.ppermute(value, axis, [(source, source + steps) for source in range(first, last)])


def swapped(value, axis, mask):
    count = lax.axis_size(axis)
    return lax.ppermute(value, axis, [(source, source ^ mask) for source in range(count)])


def bits_of(count):
    return [1 << bit for bit in range(count.bit_length() - 1)]


def attend(queries, keys, values, documents, sinks):
    rows = queries.shape[0]
    kv_heads = keys.shape[1] // HD
    group = queries.shape[1] // HD // kv_heads
    blocks = rows // WINDOW
    key_value = jnp.concatenate([keys, values], axis=1)
    tail_pair, tail_docs = passed_along(
        (key_value[rows - WINDOW :], documents[rows - WINDOW :].astype(jnp.bfloat16)), "sp", 1
    )
    ext_pair = jnp.concatenate([tail_pair, key_value], axis=0).reshape(
        blocks + 1, WINDOW, 2 * kv_heads * HD
    )
    ext_docs = jnp.concatenate([tail_docs.astype(jnp.int32), documents], axis=0).reshape(
        blocks + 1, WINDOW
    )
    band = jnp.concatenate([ext_pair[:-1], ext_pair[1:]], axis=1)
    band_keys = band[:, :, : kv_heads * HD].reshape(blocks, 2 * WINDOW, kv_heads, HD)
    band_values = band[:, :, kv_heads * HD :].reshape(blocks, 2 * WINDOW, kv_heads, HD)
    band_docs = jnp.concatenate([ext_docs[:-1], ext_docs[1:]], axis=1)
    query_docs = documents.reshape(blocks, WINDOW)
    offset = lax.axis_index("sp") * rows
    distance = jnp.arange(WINDOW)[:, None] + WINDOW - jnp.arange(2 * WINDOW)[None, :]
    key_pos = (
        offset + jnp.arange(blocks)[:, None] * WINDOW + jnp.arange(2 * WINDOW)[None, :] - WINDOW
    )
    visible = (
        ((distance >= 0) & (distance < WINDOW))[None]
        & (key_pos >= 0)[:, None, :]
        & (band_docs[:, None, :] == query_docs[:, :, None])
    )
    query_blocks = queries.reshape(blocks, WINDOW, kv_heads, group, HD)
    scores = jnp.einsum(
        "nikgd,njkd->nkgij", query_blocks, band_keys, preferred_element_type=jnp.float32
    ) * HD ** (-0.5)
    scores = jnp.where(visible[:, None, None], scores, -jnp.inf)
    sink_logit = sinks.reshape(kv_heads, group)[None, :, :, None, None]
    row_top = jnp.maximum(jnp.max(scores, axis=-1, keepdims=True), sink_logit)
    raw_weights = jnp.exp(scores - row_top)
    totals = jnp.sum(raw_weights, axis=-1, keepdims=True) + jnp.exp(sink_logit - row_top)
    weights = (raw_weights / totals).astype(jnp.bfloat16)
    attended = jnp.einsum(
        "nkgij,njkd->nikgd", weights, band_values, preferred_element_type=jnp.float32
    )
    return attended.astype(jnp.bfloat16).reshape(rows, kv_heads * group * HD)


def norm_rows(mid_rows, norm_gain):
    scale = lax.rsqrt(jnp.mean(mid_rows * mid_rows, axis=-1, keepdims=True) + 1e-06)
    return (mid_rows * scale * norm_gain).astype(jnp.bfloat16)


def by_place(pieces, me):
    for bit in bits_of(len(pieces)):
        flip = (me & bit) != 0
        pieces = [jnp.where(flip, pieces[r ^ bit], pieces[r]) for r in range(len(pieces))]
    return pieces


def own_rows(attended):
    count = lax.axis_size("tp")
    me = lax.axis_index("tp")
    rows = attended.shape[0] // count
    pieces = []
    for mask in range(count):
        piece = lax.dynamic_slice_in_dim(attended, (me ^ mask) * rows, rows)
        pieces.append(swapped(piece, "tp", mask) if mask else piece)
    return jnp.concatenate(by_place(pieces, me), axis=1)


def regrouped(gate_proj, up_proj, down_proj):
    me = lax.axis_index("sp") % SHARE
    width = gate_proj.shape[1] // SHARE
    gate_up, down = [], []
    for mask in range(SHARE):
        start = (me ^ mask) * width
        piece = jnp.concatenate(
            [
                lax.dynamic_slice_in_dim(gate_proj, start, width, axis=1),
                lax.dynamic_slice_in_dim(up_proj, start, width, axis=1),
            ],
            axis=1,
        )
        gate_up.append(swapped(piece, "sp", mask) if mask else piece)
    for mask in range(SHARE):
        piece = lax.dynamic_slice_in_dim(down_proj, (me ^ mask) * width, width, axis=0)
        down.append(swapped(piece, "sp", mask) if mask else piece)
    return (
        jnp.concatenate(by_place(gate_up, me), axis=0),
        jnp.concatenate(by_place(down, me), axis=1),
    )


def spread(chunk):
    groups = lax.axis_size("sp") // SHARE
    if groups == 4:
        half = chunk.shape[0] // 2
        low = swapped(chunk, "sp", SHARE)
        wrap = swapped(chunk, "sp", 3 * SHARE)
        first = swapped(low[:half], "sp", 3 * SHARE)
        second = swapped(wrap[half:], "sp", SHARE)
        return [chunk, low, jnp.concatenate([first, second], axis=0), wrap]
    chunks = [chunk]
    for bit in bits_of(groups):
        chunks = chunks + [swapped(piece, "sp", SHARE * bit) for piece in chunks]
    return chunks


def gathered(rows, hops):
    for axis, mask in hops:
        rows = jnp.concatenate([rows, swapped(rows, axis, mask)], axis=0)
    return rows


def scattered(partial, hops):
    total = partial
    for axis, mask in reversed(hops):
        half = total.shape[0] // 2
        arrived = swapped(total[half:].astype(jnp.bfloat16), axis, mask)
        total = total[:half].astype(jnp.float32) + arrived.astype(jnp.float32)
    return total


def shards(
    resid,
    queries,
    keys,
    values,
    documents,
    sinks,
    out_proj,
    norm_gain,
    gate_proj,
    up_proj,
    down_proj,
):
    groups = lax.axis_size("sp") // SHARE
    group = lax.axis_index("sp") // SHARE
    gate_up, down = regrouped(gate_proj, up_proj, down_proj)
    gate_up = jnp.concatenate(spread(gate_up), axis=0)
    down = jnp.concatenate(spread(down), axis=1)
    units = down.shape[0]

    attended = attend(queries, keys, values, documents, sinks)
    mid_rows = resid.astype(jnp.float32) + jnp.dot(
        own_rows(attended), out_proj, preferred_element_type=jnp.float32
    )
    normed = norm_rows(mid_rows, norm_gain)
    rows, width = normed.shape
    block = width // groups
    normed = jnp.concatenate(
        [lax.dynamic_slice_in_dim(normed, (group ^ k) * block, block, axis=1) for k in range(groups)],
        axis=1,
    )
    x_hops = [("tp", bit) for bit in bits_of(lax.axis_size("tp"))]
    y_hops = [("sp", 2)]
    core_hops = [("sp", 1)]
    sums = []
    for stream, hops in enumerate((x_hops + y_hops + core_hops, y_hops + x_hops + core_hops)):
        part = normed[stream * rows // 2 : (stream + 1) * rows // 2]
        part = gathered(part, hops)
        acts = jnp.dot(part, gate_up, preferred_element_type=jnp.float32)
        hidden = (jax.nn.silu(acts[:, :units]) * acts[:, units:]).astype(jnp.bfloat16)
        partial = jnp.dot(hidden, down, preferred_element_type=jnp.float32).astype(jnp.bfloat16)
        sums.append(scattered(partial, hops))
    summed = jnp.concatenate(sums, axis=0)
    stack = jnp.stack([summed[:, k * block : (k + 1) * block] for k in range(groups)])
    summed = jnp.concatenate(
        [lax.dynamic_index_in_dim(stack, group ^ k, keepdims=False) for k in range(groups)], axis=1
    )
    return (mid_rows + summed).astype(jnp.bfloat16)


MESH = pl.DeviceIdType.MESH
CHAIN, SIDE, CORES = 4, 2, 2


def fits(mesh):
    return mesh.shape["sp"] == CHAIN * SIDE * CORES and mesh.shape["tp"] == 2


def layer_kernel(
    documents_ref,
    gain_ref,
    sinks_ref,
    resid_hbm,
    queries_hbm,
    keys_hbm,
    values_hbm,
    out_proj_hbm,
    gate_hbm,
    up_hbm,
    down_hbm,
    out_ref,
    out_v,
    q_v,
    k_v,
    v_v,
    halo_docs,
    resid_v,
    out_proj_v,
    att,
    att_out,
    mid,
    tok,
    gu,
    dn,
    acts,
    hid,
    part,
    x_out,
    x_in,
    z_out,
    z_in,
    local_sem,
    halo_s,
    halo_r,
    own_s,
    own_r,
    tok_s,
    tok_r,
    wl,
    wz_s,
    wz_r,
    wy_s,
    wy_r,
    wc_s,
    wc_r,
    rx_s,
    rx_r,
    rz_s,
    rz_r,
    out_sem,
):
    sp = lax.axis_index("sp")
    x = lax.axis_index("tp")
    z = sp // (SIDE * CORES)
    y = (sp // CORES) % SIDE
    c = sp % CORES
    hi, lo = z // 2, z % 2
    pair = z + 1 - 2 * lo
    far_mid = 2 - hi
    far_end = 3 - 3 * hi
    is_mid = jnp.where((z == 1) | (z == 2), 1, 0)

    def at(zz, yy, cc, xx):
        return ((zz * SIDE + yy) * CORES + cc, xx)

    to_pair, to_mid, to_end = at(pair, y, c, x), at(far_mid, y, c, x), at(far_end, y, c, x)
    to_y, to_c, to_x = at(z, 1 - y, c, x), at(z, y, 1 - c, x), (sp, 1 - x)
    count = CHAIN * SIDE * CORES
    to_next = (lax.rem(sp + 1, count), x)
    to_prev = (lax.rem(sp + count - 1, count), x)

    rows, own = q_v.shape[0], resid_v.shape[0]
    depth = gate_hbm.shape[0]
    units = gu.shape[2]
    width = mid.shape[1]
    heads = sinks_ref.shape[0]
    kv_heads = k_v.shape[1] // HD
    group = heads // kv_heads
    blocks = rows // WINDOW
    pane = dn.shape[2]
    cols = heads * HD

    def remote(src, dst, send, recv, device):
        return pltpu.make_async_remote_copy(
            src_ref=src, dst_ref=dst, send_sem=send, recv_sem=recv, device_id=device, device_id_type=MESH
        )

    fetch = [
        pltpu.make_async_copy(queries_hbm, q_v, local_sem.at[0]),
        pltpu.make_async_copy(keys_hbm, k_v.at[pl.ds(WINDOW, rows), :], local_sem.at[1]),
        pltpu.make_async_copy(values_hbm, v_v.at[pl.ds(WINDOW, rows), :], local_sem.at[2]),
        pltpu.make_async_copy(resid_hbm, resid_v, local_sem.at[3]),
        pltpu.make_async_copy(out_proj_hbm, out_proj_v, local_sem.at[4]),
    ]
    for copy in fetch:
        copy.start()

    barrier = pltpu.get_barrier_semaphore()
    around = (to_pair, to_mid, to_end, to_y, to_c, to_x, to_next, to_prev)
    for device in around:
        pl.semaphore_signal(barrier, inc=1, device_id=device, device_id_type=MESH)
    pl.semaphore_wait(barrier, len(around))

    last = pl.ds(rows - WINDOW, WINDOW)
    halo = [
        remote(keys_hbm.at[last, :], k_v.at[pl.ds(0, WINDOW), :], halo_s.at[0], halo_r.at[0], to_next),
        remote(values_hbm.at[last, :], v_v.at[pl.ds(0, WINDOW), :], halo_s.at[1], halo_r.at[1], to_next),
        remote(documents_ref.at[pl.ds(blocks - 1, 1), :], halo_docs, halo_s.at[2], halo_r.at[2], to_next),
    ]
    for copy in halo:
        copy.start()

    mid_plane = is_mid == 1
    rows_z = (z, jnp.where(mid_plane, far_end, pair), far_mid, jnp.where(mid_plane, pair, far_end))
    cols_z = (z, far_mid, pair, far_end)
    z_of = (rows_z, rows_z, cols_z) + (rows_z,) * 8
    row_slots = (
        jnp.where(mid_plane, 1, 3),
        jnp.where(mid_plane, 2, 1),
        jnp.where(mid_plane, 2, 3),
    )
    col_slots = (2, jnp.where(mid_plane, 1, 3), jnp.where(mid_plane, 1, 3))
    quarters = tuple((q * depth // 4, depth // 4) for q in range(4))
    spans_of = ((0, depth), (0, depth), None) + quarters + quarters
    array_of = (0, 1, 2) + (0,) * 4 + (1,) * 4
    late = tuple(range(3, 11))

    def z_flag(kind, slot):
        return kind + 4 if kind > 2 else 3 + slot if kind == 2 else 2 * (slot - 1) + kind

    def y_flag(kind, slot):
        return kind + 7 if kind > 2 else 6 + slot if kind == 2 else 2 * slot + kind

    def c_flag(kind, slot):
        return 3 + (kind > 6) if kind > 2 else 5 + slot if kind == 2 else slot

    def place(kind, zz, yy, cc):
        if kind == 2:
            return dn.at[zz * SIDE + yy, :, pl.ds(pl.multiple_of(cc * depth, depth), depth)]
        source = (zz * SIDE + yy) * CORES + cc
        first, count = spans_of[kind]
        return gu.at[array_of[kind], pl.ds(pl.multiple_of(source * depth + first, count), count), :]

    def shard(kind, half):
        start = pl.ds(pl.multiple_of(half * units, WINDOW), units)
        if kind == 2:
            return down_hbm.at[start, :]
        return (gate_hbm, up_hbm)[array_of[kind]].at[pl.ds(*spans_of[kind]), start]

    def z_send(kind, dest):
        half, device = ((1 - lo, to_pair), (hi, to_mid), (1 - hi, to_end))[dest]
        slot = (col_slots if kind == 2 else row_slots)[dest]
        return remote(
            shard(kind, half), place(kind, z, y, c), wz_s.at[0], wz_r.at[z_flag(kind, slot)], device
        )

    def z_arrival(kind, slot):
        where = place(kind, z_of[kind][slot], y, c)
        return remote(where, where, wz_s.at[0], wz_r.at[z_flag(kind, slot)], to_pair)

    def y_send(kind, slot):
        where = place(kind, z_of[kind][slot], y, c)
        return remote(
            shard(kind, lo) if slot == 0 else where, where, wy_s.at[0], wy_r.at[y_flag(kind, slot)], to_y
        )

    def y_arrival(kind, slot):
        where = place(kind, z_of[kind][slot], 1 - y, c)
        return remote(where, where, wy_s.at[0], wy_r.at[y_flag(kind, slot)], to_y)

    def c_send(kind, slot, other):
        where = place(kind, z_of[kind][slot], 1 - y if other else y, c)
        source = shard(kind, lo) if slot == 0 and not other else where
        return remote(source, where, wc_s.at[0], wc_r.at[c_flag(kind, slot)], to_c)

    kept = [
        pltpu.make_async_copy(shard(kind, lo), place(kind, z, y, c), wl.at[kind]) for kind in range(3)
    ]

    def z_in_and_on(kind, slot):
        z_arrival(kind, slot).wait_recv()
        y_send(kind, slot).start()
        c_send(kind, slot, 0).start()

    def y_in_and_on(kind, slot):
        y_arrival(kind, slot).wait_recv()
        c_send(kind, slot, 1).start()

    @pl.when(is_mid == 1)
    def _():
        for kind in (0, 1):
            z_send(kind, 0).start()

    @pl.when(is_mid == 0)
    def _():
        for kind in (0, 1):
            z_send(kind, 1).start()

    for kind in (0, 1):
        y_send(kind, 0).start()
        c_send(kind, 0, 0).start()
    c_send(2, 0, 0).start()

    for copy in kept:
        copy.start()

    for copy in fetch[:3]:
        copy.wait()

    row = lax.broadcasted_iota(jnp.int32, (WINDOW, 2 * WINDOW), 0)
    col = lax.broadcasted_iota(jnp.int32, (WINDOW, 2 * WINDOW), 1)
    distance = row + WINDOW - col
    in_window = (distance >= 0) & (distance < WINDOW)

    def attend_block(block, target, target_row, target_col, may_be_first):
        here = documents_ref[pl.ds(block, 1), :]
        back = documents_ref[pl.ds(jnp.maximum(block - 1, 0), 1), :]
        if may_be_first:
            back = jnp.where(block == 0, halo_docs[...], back)
        band = jnp.concatenate([back, here], axis=1).astype(jnp.float32)
        mine = jnp.broadcast_to(here.astype(jnp.float32), (WINDOW, WINDOW)).T
        mine = jnp.concatenate([mine, mine], axis=1)
        visible = in_window & (band == mine)
        if may_be_first:
            visible = visible & (col >= jnp.where((sp == 0) & (block == 0), WINDOW, 0))
        start = pl.multiple_of(block * WINDOW, WINDOW)
        for kv in range(kv_heads):
            k_band = k_v[pl.ds(start, 2 * WINDOW), kv * HD : (kv + 1) * HD]
            v_band = v_v[pl.ds(start, 2 * WINDOW), kv * HD : (kv + 1) * HD]
            pieces = []
            for head in range(kv * group, (kv + 1) * group):
                q = q_v[pl.ds(start, WINDOW), head * HD : (head + 1) * HD]
                scores = lax.dot_general(
                    q, k_band, (((1,), (1,)), ((), ())), preferred_element_type=jnp.float32
                ) * HD ** (-0.5)
                scores = jnp.where(visible, scores, -jnp.inf)
                sink = sinks_ref[head]
                top = jnp.maximum(jnp.max(scores, axis=1, keepdims=True), sink)
                raw = jnp.exp(scores - top)
                total = jnp.sum(raw, axis=1, keepdims=True) + jnp.exp(sink - top)
                weights = (raw / total).astype(jnp.bfloat16)
                pieces.append(jnp.dot(weights, v_band, preferred_element_type=jnp.float32))
            merged = jnp.concatenate(pieces, axis=1).astype(jnp.bfloat16)
            at_col = target_col + kv * group * HD
            if not isinstance(at_col, int):
                at_col = pl.multiple_of(at_col, WINDOW)
            target[pl.ds(target_row, WINDOW), pl.ds(at_col, group * HD)] = merged

    own_blocks = own // WINDOW
    my_cols = pl.ds(pl.multiple_of(x * cols, WINDOW), cols)

    def own_send(part_index):
        part_rows = pl.ds(part_index * WINDOW, WINDOW)
        return remote(
            att_out.at[part_rows, :],
            att.at[part_rows, my_cols],
            own_s.at[0],
            own_r.at[part_index],
            to_x,
        )

    for b in reversed(range(own_blocks)):
        if b == 0:
            for copy in halo:
                copy.wait_recv()
        attend_block((1 - x) * own_blocks + b, att_out, b * WINDOW, 0, b == 0)
        own_send(b).start()
        attend_block(x * own_blocks + b, att, b * WINDOW, x * cols, b == 0)

    their_cols = pl.ds(pl.multiple_of((1 - x) * cols, WINDOW), cols)

    for copy in fetch[3:]:
        copy.wait()
    square = jnp.zeros((own, 1), jnp.float32)
    step = 2 * pane
    my_rows = pl.ds(pl.multiple_of(x * cols, WINDOW), cols)
    their_rows = pl.ds(pl.multiple_of((1 - x) * cols, WINDOW), cols)
    for n in range(width // step):
        block_cols = pl.ds(n * step, step)
        mid[:, block_cols] = resid_v[:, block_cols].astype(jnp.float32) + jnp.dot(
            att[:, my_cols], out_proj_v[my_rows, block_cols], preferred_element_type=jnp.float32
        )
    for b in range(own_blocks):
        where = att.at[pl.ds(b * WINDOW, WINDOW), their_cols]
        remote(where, where, own_s.at[0], own_r.at[b], to_x).wait_recv()
    for n in range(width // step):
        block_cols = pl.ds(n * step, step)
        value = mid[:, block_cols] + jnp.dot(
            att[:, their_cols], out_proj_v[their_rows, block_cols], preferred_element_type=jnp.float32
        )
        mid[:, block_cols] = value
        square = square + jnp.sum(value * value, axis=1, keepdims=True)
    scale = lax.rsqrt(square * (1.0 / width) + 1e-06)
    for n in range(width // step):
        block_cols = pl.ds(n * step, step)
        tok[pl.ds(0, own), block_cols] = (
            mid[:, block_cols] * scale * gain_ref[:, block_cols]
        ).astype(jnp.bfloat16)

    bits = own // 2

    def tok_at(slot, bit):
        return tok.at[pl.ds(slot * own + bit * bits, bits), :]

    tok_z = [remote(tok_at(0, i), tok_at(3, i), tok_s.at[0], tok_r.at[0, i], to_pair) for i in range(2)]
    tok_x = [remote(tok_at(0, i), tok_at(1, i), tok_s.at[0], tok_r.at[1, i], to_x) for i in range(2)]
    tok_on = [remote(tok_at(3, i), tok_at(2, i), tok_s.at[0], tok_r.at[2, i], to_x) for i in range(2)]
    for i in range(2):
        tok_z[i].start()
        tok_x[i].start()

    @pl.when(is_mid == 1)
    def _():
        for dest in (2, 1):
            for kind in (0, 1):
                z_send(kind, dest).start()
        z_send(2, 1).start()

    @pl.when(is_mid == 0)
    def _():
        for dest in (0, 2):
            for kind in late:
                z_send(kind, dest).start()
        z_send(2, 0).start()

    def landed(where, semaphore):
        remote(where, where, wc_s.at[0], semaphore, to_c).wait_recv()

    def ready_rows(slot):
        landed(gu.at[:, pl.ds(0, 2 * depth), :], wc_r.at[slot])

    def ready_gate():
        landed(gu.at[0, pl.ds(0, 2 * depth), :], wc_r.at[3])

    def ready_up():
        landed(gu.at[1, pl.ds(0, 2 * depth), :], wc_r.at[4])

    def ready_down(slot):
        landed(dn.at[0], wc_r.at[5 + slot])

    tall = own * 4

    def gate_up(slot, spans, first=False, final=None, kinds=(0, 1)):
        source = z_of[0][slot] * (SIDE * CORES * depth)
        deep = pl.ds(pl.multiple_of(source, SIDE * CORES * depth), SIDE * CORES * depth)

        def tile(start, size):
            at_units = pl.ds(start, size)
            for position, (at_row, height) in enumerate(spans):
                span = pl.ds(at_row, height)
                sums = []
                for kind in kinds:
                    value = jnp.dot(
                        tok[span, deep], gu[kind, deep, at_units], preferred_element_type=jnp.float32
                    )
                    if not first:
                        value = value + acts[kind, span, at_units]
                    if final is None:
                        acts[kind, span, at_units] = value
                    sums.append(value)
                if final is not None:
                    gate_acts = sums[0] if len(kinds) == 2 else acts[0, span, at_units]
                    hid[pl.ds(final + position * height, height), at_units] = (
                        gate_acts / (1.0 + jnp.exp(-gate_acts)) * value
                    ).astype(jnp.bfloat16)

        whole = units // pane

        def body(n, carry):
            tile(pl.multiple_of(n * pane, pane), pane)
            return carry

        lax.fori_loop(0, whole, body, 0)
        if units % pane:
            tile(whole * pane, units % pane)

    def gate_only(slot):
        gate_up(slot, sent, kinds=(0,))

    def last_up(slot, spans, final):
        gate_up(slot, spans, final=final, kinds=(1,))

    half = tall // 2
    near, theirs, paired = ((0, half),), ((half, own),), ((half + own, own),)
    far = ((half, half),)
    sent, held = ((own, half),), ((0, own), (tall - own, own))

    panes = [(slot, other) for slot in range(4) for other in range(2)]
    pair_first = (3,)

    def pane_of(i):
        slot, other = panes[i]
        return z_of[2][slot] * SIDE + (1 - y if other else y)

    whole_rows = {0: pl.ds(0, own), 1: pl.ds(own, own)}

    def first_hop(i, relayed):
        j = pane_of(i)
        device = to_pair if i in pair_first else to_x
        taken = whole_rows[relayed]
        return remote(
            x_out.at[j, taken, :], x_in.at[j, taken, :], rx_s.at[0], rx_r.at[i, relayed], device
        )

    def second_hop(i):
        j = pane_of(i)
        device = to_x if i in pair_first else to_pair
        return remote(z_out.at[j], z_in.at[j], rz_s.at[0], rz_r.at[j], device)

    def down_sent(i):
        j = pane_of(i)
        x_out[j] = jnp.dot(
            hid[pl.ds(0, half), :], dn[j], preferred_element_type=jnp.float32
        ).astype(jnp.bfloat16)
        first_hop(i, 1).start()

    def down_held(i):
        j = pane_of(i)
        part[j] = jnp.dot(hid[pl.ds(half, half), :], dn[j], preferred_element_type=jnp.float32)

    def down_both(i):
        j = pane_of(i)
        partial = jnp.dot(hid[...], dn[j], preferred_element_type=jnp.float32)
        x_out[j, whole_rows[0], :] = partial[3 * own :, :].astype(jnp.bfloat16)
        x_out[j, whole_rows[1], :] = partial[own : 2 * own, :].astype(jnp.bfloat16)
        first_hop(i, 1).start()
        part[j, whole_rows[0], :] = partial[2 * own : 3 * own, :]
        part[j, whole_rows[1], :] = partial[:own, :]

    def send_rest(*given):
        for i in given:
            first_hop(i, 0).start()

    def relay(i):
        j = pane_of(i)
        first_hop(i, 1).wait_recv()
        z_out[j] = (part[j, whole_rows[1], :] + x_in[j, whole_rows[1], :].astype(jnp.float32)).astype(
            jnp.bfloat16
        )
        second_hop(i).start()

    def store(i):
        at_cols = pl.ds(pl.multiple_of(pane_of(i) * pane, pane), pane)
        return pltpu.make_async_copy(out_v.at[:, at_cols], out_ref.at[:, at_cols], out_sem.at[0])

    def finish(i):
        j = pane_of(i)
        first_hop(i, 0).wait_recv()
        second_hop(i).wait_recv()
        at_cols = pl.ds(pl.multiple_of(j * pane, pane), pane)
        summed = part[j, whole_rows[0], :] + x_in[j, whole_rows[0], :].astype(jnp.float32)
        out_v[:, at_cols] = (mid[:, at_cols] + (summed + z_in[j].astype(jnp.float32))).astype(
            jnp.bfloat16
        )
        store(i).start()

    def tok_forward(i):
        tok_z[i].wait_recv()
        tok_on[i].start()

    def tok_wait(group):
        for copy in group:
            copy.wait_recv()

    def late_down(dest):
        z_send(2, dest).start()

    def own_down():
        y_send(2, 0).start()

    def apart(ends, mids):
        for want, listed in ((0, ends), (1, mids)):

            @pl.when(is_mid == want)
            def _():
                run(listed)

    def kept_wait(kind):
        kept[kind].wait()

    def settle():
        for copy in halo:
            copy.wait_send()
        for where, semaphore in (
            (att_out, own_s),
            (tok.at[pl.ds(0, 3 * own), :], tok_s),
            (gu.at[0, pl.ds(0, 9 * depth), :], wz_s),
            (gu.at[0, pl.ds(0, 12 * depth), :], wy_s),
            (gu.at[:, pl.ds(0, 12 * depth), :], wc_s),
        ):
            remote(where, where, semaphore.at[0], halo_r.at[0], to_x).wait_send()

    def z_late(*kinds):
        for kind in kinds:
            z_in_and_on(kind, 3)

    def y_late(*kinds):
        for kind in kinds:
            y_in_and_on(kind, 3)

    steps = (
        (y_in_and_on, 0, 0),
        (z_in_and_on, 0, 1),
        (y_in_and_on, 1, 0),
        (z_in_and_on, 1, 1),
        (y_in_and_on, 0, 1),
        (
            apart,
            ((z_in_and_on, 0, 2), (y_in_and_on, 1, 1), (z_in_and_on, 1, 2)),
            ((tok_forward, 0), (y_in_and_on, 1, 1), (own_down,), (tok_forward, 1), (z_in_and_on, 0, 2)),
        ),
        (tok_wait, tok_x),
        (kept_wait, 0),
        (kept_wait, 1),
        (ready_rows, 0),
        (gate_up, 0, near, True),
        (apart, (), ((z_late, 3, 4),)),
        (ready_rows, 1),
        (gate_up, 1, near),
        (
            apart,
            (
                (y_in_and_on, 0, 2),
                (tok_forward, 0),
                (own_down,),
                (y_in_and_on, 1, 2),
                (tok_forward, 1),
            ),
            ((z_late, 5, 6), (z_in_and_on, 1, 2)),
        ),
        (gate_up, 0, paired, True),
        (
            apart,
            ((ready_rows, 2), (gate_up, 2, near), (z_late, 3, 4)),
            ((z_late, 7, 8), (y_in_and_on, 0, 2)),
        ),
        (gate_up, 1, paired),
        (
            apart,
            ((z_late, 5), (gate_up, 2, paired), (z_late, 6, 7)),
            ((z_late, 9, 10), (y_late, 3, 4)),
        ),
        (tok_wait, tok_on),
        (gate_up, 0, theirs, True),
        (apart, ((z_late, 8), (y_late, 3, 4)), ((y_late, 5, 6),)),
        (gate_up, 1, theirs),
        (
            apart,
            ((z_late, 9), (y_late, 5, 6), (z_late, 10), (gate_up, 2, theirs), (ready_gate,), (gate_only, 3)),
            (
                (late_down, 2),
                (y_in_and_on, 1, 2),
                (ready_gate,),
                (gate_only, 3),
                (ready_rows, 2),
                (gate_up, 2, near),
                (late_down, 0),
                (y_late, 7, 8),
                (gate_up, 2, far),
            ),
        ),
        (apart, ((y_late, 7, 8),), ()),
        (y_in_and_on, 2, 0),
        (y_late, 9, 10),
        (ready_up,),
        (last_up, 3, sent, 0),
        (kept_wait, 2),
        (ready_down, 0),
        (down_sent, 0),
        (apart, ((late_down, 1), (late_down, 2)), ()),
        (z_in_and_on, 2, 1),
        (send_rest, 0),
        (down_sent, 1),
        (send_rest, 1),
        (gate_up, 3, held, False, half),
        (z_in_and_on, 2, 2),
        (down_held, 0),
        (y_in_and_on, 2, 1),
        (down_held, 1),
        (ready_down, 1),
        (down_sent, 2),
        (send_rest, 2),
        (down_both, 3),
        (send_rest, 3),
        (relay, 0),
        (relay, 1),
        (y_in_and_on, 2, 2),
        (ready_down, 2),
        (down_sent, 4),
        (send_rest, 4),
        (z_in_and_on, 2, 3),
        (down_sent, 5),
        (send_rest, 5),
        (down_held, 2),
        (relay, 2),
        (relay, 3),
        (y_in_and_on, 2, 3),
        (ready_down, 3),
        (down_sent, 6),
        (down_sent, 7),
        (send_rest, 6, 7),
        (down_held, 4),
        (relay, 4),
        (down_held, 5),
        (down_held, 6),
        (relay, 5),
        (down_held, 7),
        (settle,),
        (relay, 6),
        (relay, 7),
        (finish, 0),
        (finish, 1),
        (finish, 2),
        (finish, 3),
        (finish, 4),
        (finish, 5),
        (finish, 6),
        (finish, 7),
    )

    def run(listed):
        for action, *given in listed:
            if action is apart:
                apart(*given)
                continue
            action(*given)

    run(steps)

    remote(x_out, x_out, rx_s.at[0], halo_r.at[0], to_x).wait_send()
    remote(z_out, z_out, rz_s.at[0], halo_r.at[0], to_x).wait_send()
    pltpu.make_async_copy(out_v, out_ref, out_sem.at[0]).wait()


def one_kernel(
    resid, queries, keys, values, documents, sinks, out_proj, norm_gain, gate_proj, up_proj, down_proj
):
    rows, own, width = queries.shape[0], resid.shape[0], resid.shape[1]
    units = gate_proj.shape[1] // 2
    deep = gate_proj.shape[0] * CHAIN * SIDE * CORES
    pane = gate_proj.shape[0] * CORES
    panes = width // pane
    heads_cols, kv_cols = queries.shape[1], keys.shape[1]
    bf16, f32 = jnp.bfloat16, jnp.float32
    vmem = pl.BlockSpec(memory_space=pltpu.VMEM)
    anywhere = pl.BlockSpec(memory_space=pl.ANY)
    dma = pltpu.SemaphoreType.DMA
    tall = 4 * own
    return pl.pallas_call(
        layer_kernel,
        out_shape=jax.ShapeDtypeStruct((own, width), bf16),
        in_specs=[vmem, vmem, pl.BlockSpec(memory_space=pltpu.SMEM)] + [anywhere] * 8,
        out_specs=anywhere,
        scratch_shapes=[
            pltpu.VMEM((own, width), bf16),
            pltpu.VMEM((rows, heads_cols), bf16),
            pltpu.VMEM((rows + WINDOW, kv_cols), bf16),
            pltpu.VMEM((rows + WINDOW, kv_cols), bf16),
            pltpu.VMEM((1, WINDOW), jnp.int32),
            pltpu.VMEM((own, width), bf16),
            pltpu.VMEM(out_proj.shape, bf16),
            pltpu.VMEM((own, out_proj.shape[0]), bf16),
            pltpu.VMEM((own, heads_cols), bf16),
            pltpu.VMEM((own, width), f32),
            pltpu.VMEM((tall, width), bf16),
            pltpu.VMEM((2, deep, units), bf16),
            pltpu.VMEM((panes, units, pane), bf16),
            pltpu.VMEM((2, tall, units), f32),
            pltpu.VMEM((tall, units), bf16),
            pltpu.VMEM((panes, tall // 2, pane), f32),
            pltpu.VMEM((panes, tall // 2, pane), bf16),
            pltpu.VMEM((panes, tall // 2, pane), bf16),
            pltpu.VMEM((panes, own, pane), bf16),
            pltpu.VMEM((panes, own, pane), bf16),
            dma((5,)),
            dma((3,)),
            dma((3,)),
            dma((1,)),
            dma((own // WINDOW,)),
            dma((1,)),
            dma((3, 2)),
            dma((3,)),
            dma((1,)),
            dma((15,)),
            dma((1,)),
            dma((18,)),
            dma((1,)),
            dma((9,)),
            dma((1,)),
            dma((panes, 2)),
            dma((1,)),
            dma((panes,)),
            dma((1,)),
        ],
        compiler_params=pltpu.CompilerParams(
            collective_id=0, has_side_effects=True, vmem_limit_bytes=66_000_000
        ),
        name="layer",
    )(
        documents.reshape(rows // WINDOW, WINDOW),
        norm_gain.reshape(1, width),
        sinks,
        resid,
        queries,
        keys,
        values,
        out_proj,
        gate_proj,
        up_proj,
        down_proj,
    )


def solution(mesh):
    in_specs = (
        P(("sp", "tp"), None),
        P("sp", "tp"),
        P("sp", "tp"),
        P("sp", "tp"),
        P("sp"),
        P("tp"),
        P(),
        P(),
        P("sp", "tp"),
        P("sp", "tp"),
        P("tp", "sp"),
    )
    out_specs = P(("sp", "tp"), None)
    if fits(mesh):
        program = lambda *arrays: one_kernel(*arrays)
        return jax.shard_map(
            program, mesh=mesh, in_specs=in_specs, out_specs=out_specs, check_vma=False
        )
    return jax.shard_map(shards, mesh=mesh, in_specs=in_specs, out_specs=out_specs, check_vma=False)
```

```python
import jax
import jax.numpy as jnp
from jax import lax
from jax.experimental import pallas as pl
from jax.experimental.pallas import tpu as pltpu
from jax.sharding import PartitionSpec as P

HD = 64
WINDOW = 128
SHARE = 4


def passed_along(value, axis, steps):
    count = lax.axis_size(axis)
    first, last = (max(0, -steps), min(count, count - steps))
    return lax.ppermute(value, axis, [(source, source + steps) for source in range(first, last)])


def swapped(value, axis, mask):
    count = lax.axis_size(axis)
    return lax.ppermute(value, axis, [(source, source ^ mask) for source in range(count)])


def bits_of(count):
    return [1 << bit for bit in range(count.bit_length() - 1)]


def attend(queries, keys, values, documents, sinks):
    rows = queries.shape[0]
    kv_heads = keys.shape[1] // HD
    group = queries.shape[1] // HD // kv_heads
    blocks = rows // WINDOW
    key_value = jnp.concatenate([keys, values], axis=1)
    tail_pair, tail_docs = passed_along(
        (key_value[rows - WINDOW :], documents[rows - WINDOW :].astype(jnp.bfloat16)), "sp", 1
    )
    ext_pair = jnp.concatenate([tail_pair, key_value], axis=0).reshape(
        blocks + 1, WINDOW, 2 * kv_heads * HD
    )
    ext_docs = jnp.concatenate([tail_docs.astype(jnp.int32), documents], axis=0).reshape(
        blocks + 1, WINDOW
    )
    band = jnp.concatenate([ext_pair[:-1], ext_pair[1:]], axis=1)
    band_keys = band[:, :, : kv_heads * HD].reshape(blocks, 2 * WINDOW, kv_heads, HD)
    band_values = band[:, :, kv_heads * HD :].reshape(blocks, 2 * WINDOW, kv_heads, HD)
    band_docs = jnp.concatenate([ext_docs[:-1], ext_docs[1:]], axis=1)
    query_docs = documents.reshape(blocks, WINDOW)
    offset = lax.axis_index("sp") * rows
    distance = jnp.arange(WINDOW)[:, None] + WINDOW - jnp.arange(2 * WINDOW)[None, :]
    key_pos = (
        offset + jnp.arange(blocks)[:, None] * WINDOW + jnp.arange(2 * WINDOW)[None, :] - WINDOW
    )
    visible = (
        ((distance >= 0) & (distance < WINDOW))[None]
        & (key_pos >= 0)[:, None, :]
        & (band_docs[:, None, :] == query_docs[:, :, None])
    )
    query_blocks = queries.reshape(blocks, WINDOW, kv_heads, group, HD)
    scores = jnp.einsum(
        "nikgd,njkd->nkgij", query_blocks, band_keys, preferred_element_type=jnp.float32
    ) * HD ** (-0.5)
    scores = jnp.where(visible[:, None, None], scores, -jnp.inf)
    sink_logit = sinks.reshape(kv_heads, group)[None, :, :, None, None]
    row_top = jnp.maximum(jnp.max(scores, axis=-1, keepdims=True), sink_logit)
    raw_weights = jnp.exp(scores - row_top)
    totals = jnp.sum(raw_weights, axis=-1, keepdims=True) + jnp.exp(sink_logit - row_top)
    weights = (raw_weights / totals).astype(jnp.bfloat16)
    attended = jnp.einsum(
        "nkgij,njkd->nikgd", weights, band_values, preferred_element_type=jnp.float32
    )
    return attended.astype(jnp.bfloat16).reshape(rows, kv_heads * group * HD)


def norm_rows(mid_rows, norm_gain):
    scale = lax.rsqrt(jnp.mean(mid_rows * mid_rows, axis=-1, keepdims=True) + 1e-06)
    return (mid_rows * scale * norm_gain).astype(jnp.bfloat16)


def by_place(pieces, me):
    for bit in bits_of(len(pieces)):
        flip = (me & bit) != 0
        pieces = [jnp.where(flip, pieces[r ^ bit], pieces[r]) for r in range(len(pieces))]
    return pieces


def own_rows(attended):
    count = lax.axis_size("tp")
    me = lax.axis_index("tp")
    rows = attended.shape[0] // count
    pieces = []
    for mask in range(count):
        piece = lax.dynamic_slice_in_dim(attended, (me ^ mask) * rows, rows)
        pieces.append(swapped(piece, "tp", mask) if mask else piece)
    return jnp.concatenate(by_place(pieces, me), axis=1)


def regrouped(gate_proj, up_proj, down_proj):
    me = lax.axis_index("sp") % SHARE
    width = gate_proj.shape[1] // SHARE
    gate_up, down = [], []
    for mask in range(SHARE):
        start = (me ^ mask) * width
        piece = jnp.concatenate(
            [
                lax.dynamic_slice_in_dim(gate_proj, start, width, axis=1),
                lax.dynamic_slice_in_dim(up_proj, start, width, axis=1),
            ],
            axis=1,
        )
        gate_up.append(swapped(piece, "sp", mask) if mask else piece)
    for mask in range(SHARE):
        piece = lax.dynamic_slice_in_dim(down_proj, (me ^ mask) * width, width, axis=0)
        down.append(swapped(piece, "sp", mask) if mask else piece)
    return (
        jnp.concatenate(by_place(gate_up, me), axis=0),
        jnp.concatenate(by_place(down, me), axis=1),
    )


def spread(chunk):
    groups = lax.axis_size("sp") // SHARE
    if groups == 4:
        half = chunk.shape[0] // 2
        low = swapped(chunk, "sp", SHARE)
        wrap = swapped(chunk, "sp", 3 * SHARE)
        first = swapped(low[:half], "sp", 3 * SHARE)
        second = swapped(wrap[half:], "sp", SHARE)
        return [chunk, low, jnp.concatenate([first, second], axis=0), wrap]
    chunks = [chunk]
    for bit in bits_of(groups):
        chunks = chunks + [swapped(piece, "sp", SHARE * bit) for piece in chunks]
    return chunks


def gathered(rows, hops):
    for axis, mask in hops:
        rows = jnp.concatenate([rows, swapped(rows, axis, mask)], axis=0)
    return rows


def scattered(partial, hops):
    total = partial
    for axis, mask in reversed(hops):
        half = total.shape[0] // 2
        arrived = swapped(total[half:].astype(jnp.bfloat16), axis, mask)
        total = total[:half].astype(jnp.float32) + arrived.astype(jnp.float32)
    return total


def shards(
    resid,
    queries,
    keys,
    values,
    documents,
    sinks,
    out_proj,
    norm_gain,
    gate_proj,
    up_proj,
    down_proj,
):
    groups = lax.axis_size("sp") // SHARE
    group = lax.axis_index("sp") // SHARE
    gate_up, down = regrouped(gate_proj, up_proj, down_proj)
    gate_up = jnp.concatenate(spread(gate_up), axis=0)
    down = jnp.concatenate(spread(down), axis=1)
    units = down.shape[0]

    attended = attend(queries, keys, values, documents, sinks)
    mid_rows = resid.astype(jnp.float32) + jnp.dot(
        own_rows(attended), out_proj, preferred_element_type=jnp.float32
    )
    normed = norm_rows(mid_rows, norm_gain)
    rows, width = normed.shape
    block = width // groups
    normed = jnp.concatenate(
        [lax.dynamic_slice_in_dim(normed, (group ^ k) * block, block, axis=1) for k in range(groups)],
        axis=1,
    )
    x_hops = [("tp", bit) for bit in bits_of(lax.axis_size("tp"))]
    y_hops = [("sp", 2)]
    core_hops = [("sp", 1)]
    sums = []
    for stream, hops in enumerate((x_hops + y_hops + core_hops, y_hops + x_hops + core_hops)):
        part = normed[stream * rows // 2 : (stream + 1) * rows // 2]
        part = gathered(part, hops)
        acts = jnp.dot(part, gate_up, preferred_element_type=jnp.float32)
        hidden = (jax.nn.silu(acts[:, :units]) * acts[:, units:]).astype(jnp.bfloat16)
        partial = jnp.dot(hidden, down, preferred_element_type=jnp.float32).astype(jnp.bfloat16)
        sums.append(scattered(partial, hops))
    summed = jnp.concatenate(sums, axis=0)
    stack = jnp.stack([summed[:, k * block : (k + 1) * block] for k in range(groups)])
    summed = jnp.concatenate(
        [lax.dynamic_index_in_dim(stack, group ^ k, keepdims=False) for k in range(groups)], axis=1
    )
    return (mid_rows + summed).astype(jnp.bfloat16)


MESH = pl.DeviceIdType.MESH
CHAIN, SIDE, CORES = 4, 2, 2


def fits(mesh):
    return mesh.shape["sp"] == CHAIN * SIDE * CORES and mesh.shape["tp"] == 2


def layer_kernel(
    documents_hbm,
    gain_hbm,
    sinks_hbm,
    resid_hbm,
    queries_hbm,
    keys_hbm,
    values_hbm,
    out_proj_hbm,
    gate_hbm,
    up_hbm,
    down_hbm,
    out_ref,
    documents_ref,
    gain_ref,
    sinks_ref,
    out_v,
    q_v,
    k_v,
    v_v,
    halo_docs,
    resid_v,
    out_proj_v,
    att,
    att_out,
    mid,
    tok,
    gu,
    dn,
    acts,
    hid,
    part,
    x_out,
    x_in,
    z_out,
    z_in,
    local_sem,
    halo_s,
    halo_r,
    own_s,
    own_r,
    tok_s,
    tok_r,
    wl,
    wz_s,
    wz_r,
    wy_s,
    wy_r,
    wc_s,
    wc_r,
    rx_s,
    rx_r,
    rz_s,
    rz_r,
    out_sem,
):
    sp = lax.axis_index("sp")
    x = lax.axis_index("tp")
    z = sp // (SIDE * CORES)
    y = (sp // CORES) % SIDE
    c = sp % CORES
    hi, lo = z // 2, z % 2
    pair = z + 1 - 2 * lo
    far_mid = 2 - hi
    far_end = 3 - 3 * hi
    is_mid = jnp.where((z == 1) | (z == 2), 1, 0)

    def at(zz, yy, cc, xx):
        return ((zz * SIDE + yy) * CORES + cc, xx)

    to_pair, to_mid, to_end = at(pair, y, c, x), at(far_mid, y, c, x), at(far_end, y, c, x)
    to_y, to_c, to_x = at(z, 1 - y, c, x), at(z, y, 1 - c, x), (sp, 1 - x)
    count = CHAIN * SIDE * CORES
    to_next = (lax.rem(sp + 1, count), x)
    to_prev = (lax.rem(sp + count - 1, count), x)

    rows, own = q_v.shape[0], resid_v.shape[0]
    depth = gate_hbm.shape[0]
    units = gu.shape[2]
    width = mid.shape[1]
    heads = sinks_ref.shape[1]
    kv_heads = k_v.shape[1] // HD
    group = heads // kv_heads
    blocks = rows // WINDOW
    pane = dn.shape[2]
    cols = heads * HD

    def remote(src, dst, send, recv, device):
        return pltpu.make_async_remote_copy(
            src_ref=src, dst_ref=dst, send_sem=send, recv_sem=recv, device_id=device, device_id_type=MESH
        )

    small = [
        pltpu.make_async_copy(documents_hbm, documents_ref, local_sem.at[5]),
        pltpu.make_async_copy(gain_hbm, gain_ref, local_sem.at[6]),
        pltpu.make_async_copy(sinks_hbm, sinks_ref, local_sem.at[7]),
    ]
    fetch = [
        pltpu.make_async_copy(queries_hbm, q_v, local_sem.at[0]),
        pltpu.make_async_copy(keys_hbm, k_v.at[pl.ds(WINDOW, rows), :], local_sem.at[1]),
        pltpu.make_async_copy(values_hbm, v_v.at[pl.ds(WINDOW, rows), :], local_sem.at[2]),
        pltpu.make_async_copy(resid_hbm, resid_v, local_sem.at[3]),
        pltpu.make_async_copy(out_proj_hbm, out_proj_v, local_sem.at[4]),
    ]
    for copy in small + fetch:
        copy.start()

    barrier = pltpu.get_barrier_semaphore()
    around = (to_pair, to_mid, to_end, to_y, to_c, to_x, to_next, to_prev)
    for device in around:
        pl.semaphore_signal(barrier, inc=1, device_id=device, device_id_type=MESH)
    pl.semaphore_wait(barrier, len(around))

    last = pl.ds(rows - WINDOW, WINDOW)
    halo = [
        remote(keys_hbm.at[last, :], k_v.at[pl.ds(0, WINDOW), :], halo_s.at[0], halo_r.at[0], to_next),
        remote(values_hbm.at[last, :], v_v.at[pl.ds(0, WINDOW), :], halo_s.at[1], halo_r.at[1], to_next),
        remote(documents_ref.at[pl.ds(blocks - 1, 1), :], halo_docs, halo_s.at[2], halo_r.at[2], to_next),
    ]
    small[0].wait()
    for copy in halo:
        copy.start()

    mid_plane = is_mid == 1
    rows_z = (z, jnp.where(mid_plane, far_end, pair), far_mid, jnp.where(mid_plane, pair, far_end))
    cols_z = (z, far_mid, pair, far_end)
    z_of = (rows_z, rows_z, cols_z) + (rows_z,) * 8
    row_slots = (
        jnp.where(mid_plane, 1, 3),
        jnp.where(mid_plane, 2, 1),
        jnp.where(mid_plane, 2, 3),
    )
    col_slots = (2, jnp.where(mid_plane, 1, 3), jnp.where(mid_plane, 1, 3))
    quarters = tuple((q * depth // 4, depth // 4) for q in range(4))
    spans_of = ((0, depth), (0, depth), None) + quarters + quarters
    array_of = (0, 1, 2) + (0,) * 4 + (1,) * 4
    late = tuple(range(3, 11))

    def z_flag(kind, slot):
        return kind + 4 if kind > 2 else 3 + slot if kind == 2 else 2 * (slot - 1) + kind

    def y_flag(kind, slot):
        return kind + 7 if kind > 2 else 6 + slot if kind == 2 else 2 * slot + kind

    def c_flag(kind, slot):
        return 3 + (kind > 6) if kind > 2 else 5 + slot if kind == 2 else slot

    def place(kind, zz, yy, cc):
        if kind == 2:
            return dn.at[zz * SIDE + yy, :, pl.ds(pl.multiple_of(cc * depth, depth), depth)]
        source = (zz * SIDE + yy) * CORES + cc
        first, count = spans_of[kind]
        return gu.at[array_of[kind], pl.ds(pl.multiple_of(source * depth + first, count), count), :]

    def shard(kind, half):
        start = pl.ds(pl.multiple_of(half * units, WINDOW), units)
        if kind == 2:
            return down_hbm.at[start, :]
        return (gate_hbm, up_hbm)[array_of[kind]].at[pl.ds(*spans_of[kind]), start]

    def z_send(kind, dest):
        half, device = ((1 - lo, to_pair), (hi, to_mid), (1 - hi, to_end))[dest]
        slot = (col_slots if kind == 2 else row_slots)[dest]
        return remote(
            shard(kind, half), place(kind, z, y, c), wz_s.at[0], wz_r.at[z_flag(kind, slot)], device
        )

    def z_arrival(kind, slot):
        where = place(kind, z_of[kind][slot], y, c)
        return remote(where, where, wz_s.at[0], wz_r.at[z_flag(kind, slot)], to_pair)

    def y_send(kind, slot):
        where = place(kind, z_of[kind][slot], y, c)
        return remote(
            shard(kind, lo) if slot == 0 else where, where, wy_s.at[0], wy_r.at[y_flag(kind, slot)], to_y
        )

    def y_arrival(kind, slot):
        where = place(kind, z_of[kind][slot], 1 - y, c)
        return remote(where, where, wy_s.at[0], wy_r.at[y_flag(kind, slot)], to_y)

    def c_send(kind, slot, other):
        where = place(kind, z_of[kind][slot], 1 - y if other else y, c)
        source = shard(kind, lo) if slot == 0 and not other else where
        return remote(source, where, wc_s.at[0], wc_r.at[c_flag(kind, slot)], to_c)

    kept = [
        pltpu.make_async_copy(shard(kind, lo), place(kind, z, y, c), wl.at[kind]) for kind in range(3)
    ]

    def z_in_and_on(kind, slot):
        z_arrival(kind, slot).wait_recv()
        y_send(kind, slot).start()
        c_send(kind, slot, 0).start()

    def y_in_and_on(kind, slot):
        y_arrival(kind, slot).wait_recv()
        c_send(kind, slot, 1).start()

    @pl.when(is_mid == 1)
    def _():
        for kind in (0, 1):
            z_send(kind, 0).start()

    @pl.when(is_mid == 0)
    def _():
        for kind in (0, 1):
            z_send(kind, 1).start()

    for kind in (0, 1):
        y_send(kind, 0).start()
        c_send(kind, 0, 0).start()
    c_send(2, 0, 0).start()

    for copy in kept:
        copy.start()

    for copy in small[1:] + fetch[:3]:
        copy.wait()

    row = lax.broadcasted_iota(jnp.int32, (WINDOW, 2 * WINDOW), 0)
    col = lax.broadcasted_iota(jnp.int32, (WINDOW, 2 * WINDOW), 1)
    distance = row + WINDOW - col
    in_window = (distance >= 0) & (distance < WINDOW)

    def attend_block(block, target, target_row, target_col, may_be_first):
        here = documents_ref[pl.ds(block, 1), :]
        back = documents_ref[pl.ds(jnp.maximum(block - 1, 0), 1), :]
        if may_be_first:
            back = jnp.where(block == 0, halo_docs[...], back)
        band = jnp.concatenate([back, here], axis=1).astype(jnp.float32)
        mine = jnp.broadcast_to(here.astype(jnp.float32), (WINDOW, WINDOW)).T
        mine = jnp.concatenate([mine, mine], axis=1)
        visible = in_window & (band == mine)
        if may_be_first:
            visible = visible & (col >= jnp.where((sp == 0) & (block == 0), WINDOW, 0))
        start = pl.multiple_of(block * WINDOW, WINDOW)
        for kv in range(kv_heads):
            k_band = k_v[pl.ds(start, 2 * WINDOW), kv * HD : (kv + 1) * HD]
            v_band = v_v[pl.ds(start, 2 * WINDOW), kv * HD : (kv + 1) * HD]
            pieces = []
            for head in range(kv * group, (kv + 1) * group):
                q = q_v[pl.ds(start, WINDOW), head * HD : (head + 1) * HD]
                scores = lax.dot_general(
                    q, k_band, (((1,), (1,)), ((), ())), preferred_element_type=jnp.float32
                ) * HD ** (-0.5)
                scores = jnp.where(visible, scores, -jnp.inf)
                sink = sinks_ref[0, head]
                top = jnp.maximum(jnp.max(scores, axis=1, keepdims=True), sink)
                raw = jnp.exp(scores - top)
                total = jnp.sum(raw, axis=1, keepdims=True) + jnp.exp(sink - top)
                weights = (raw / total).astype(jnp.bfloat16)
                pieces.append(jnp.dot(weights, v_band, preferred_element_type=jnp.float32))
            merged = jnp.concatenate(pieces, axis=1).astype(jnp.bfloat16)
            at_col = target_col + kv * group * HD
            if not isinstance(at_col, int):
                at_col = pl.multiple_of(at_col, WINDOW)
            target[pl.ds(target_row, WINDOW), pl.ds(at_col, group * HD)] = merged

    own_blocks = own // WINDOW
    my_cols = pl.ds(pl.multiple_of(x * cols, WINDOW), cols)

    def own_send(part_index):
        part_rows = pl.ds(part_index * WINDOW, WINDOW)
        return remote(
            att_out.at[part_rows, :],
            att.at[part_rows, my_cols],
            own_s.at[0],
            own_r.at[part_index],
            to_x,
        )

    for b in reversed(range(own_blocks)):
        if b == 0:
            for copy in halo:
                copy.wait_recv()
        attend_block((1 - x) * own_blocks + b, att_out, b * WINDOW, 0, b == 0)
        own_send(b).start()
        attend_block(x * own_blocks + b, att, b * WINDOW, x * cols, b == 0)

    their_cols = pl.ds(pl.multiple_of((1 - x) * cols, WINDOW), cols)

    for copy in fetch[3:]:
        copy.wait()
    square = jnp.zeros((own, 1), jnp.float32)
    step = 2 * pane
    my_rows = pl.ds(pl.multiple_of(x * cols, WINDOW), cols)
    their_rows = pl.ds(pl.multiple_of((1 - x) * cols, WINDOW), cols)
    for n in range(width // step):
        block_cols = pl.ds(n * step, step)
        mid[:, block_cols] = resid_v[:, block_cols].astype(jnp.float32) + jnp.dot(
            att[:, my_cols], out_proj_v[my_rows, block_cols], preferred_element_type=jnp.float32
        )
    for b in range(own_blocks):
        where = att.at[pl.ds(b * WINDOW, WINDOW), their_cols]
        remote(where, where, own_s.at[0], own_r.at[b], to_x).wait_recv()
    for n in range(width // step):
        block_cols = pl.ds(n * step, step)
        value = mid[:, block_cols] + jnp.dot(
            att[:, their_cols], out_proj_v[their_rows, block_cols], preferred_element_type=jnp.float32
        )
        mid[:, block_cols] = value
        square = square + jnp.sum(value * value, axis=1, keepdims=True)
    scale = lax.rsqrt(square * (1.0 / width) + 1e-06)
    for n in range(width // step):
        block_cols = pl.ds(n * step, step)
        tok[pl.ds(0, own), block_cols] = (
            mid[:, block_cols] * scale * gain_ref[:, block_cols]
        ).astype(jnp.bfloat16)

    bits = own // 2

    def tok_at(slot, bit):
        return tok.at[pl.ds(slot * own + bit * bits, bits), :]

    tok_z = [remote(tok_at(0, i), tok_at(3, i), tok_s.at[0], tok_r.at[0, i], to_pair) for i in range(2)]
    tok_x = [remote(tok_at(0, i), tok_at(1, i), tok_s.at[0], tok_r.at[1, i], to_x) for i in range(2)]
    tok_on = [remote(tok_at(3, i), tok_at(2, i), tok_s.at[0], tok_r.at[2, i], to_x) for i in range(2)]
    for i in range(2):
        tok_z[i].start()
        tok_x[i].start()

    @pl.when(is_mid == 1)
    def _():
        for dest in (2, 1):
            for kind in (0, 1):
                z_send(kind, dest).start()
        z_send(2, 1).start()

    @pl.when(is_mid == 0)
    def _():
        for dest in (0, 2):
            for kind in late:
                z_send(kind, dest).start()
        z_send(2, 0).start()

    def landed(where, semaphore):
        remote(where, where, wc_s.at[0], semaphore, to_c).wait_recv()

    def ready_rows(slot):
        landed(gu.at[:, pl.ds(0, 2 * depth), :], wc_r.at[slot])

    def ready_gate():
        landed(gu.at[0, pl.ds(0, 2 * depth), :], wc_r.at[3])

    def ready_up():
        landed(gu.at[1, pl.ds(0, 2 * depth), :], wc_r.at[4])

    def ready_down(slot):
        landed(dn.at[0], wc_r.at[5 + slot])

    tall = own * 4

    def gate_up(slot, spans, first=False, final=None, kinds=(0, 1)):
        source = z_of[0][slot] * (SIDE * CORES * depth)
        deep = pl.ds(pl.multiple_of(source, SIDE * CORES * depth), SIDE * CORES * depth)

        def tile(start, size):
            at_units = pl.ds(start, size)
            for position, (at_row, height) in enumerate(spans):
                span = pl.ds(at_row, height)
                sums = []
                for kind in kinds:
                    value = jnp.dot(
                        tok[span, deep], gu[kind, deep, at_units], preferred_element_type=jnp.float32
                    )
                    if not first:
                        value = value + acts[kind, span, at_units]
                    if final is None:
                        acts[kind, span, at_units] = value
                    sums.append(value)
                if final is not None:
                    gate_acts = sums[0] if len(kinds) == 2 else acts[0, span, at_units]
                    hid[pl.ds(final + position * height, height), at_units] = (
                        gate_acts / (1.0 + jnp.exp(-gate_acts)) * value
                    ).astype(jnp.bfloat16)

        whole = units // pane

        def body(n, carry):
            tile(pl.multiple_of(n * pane, pane), pane)
            return carry

        lax.fori_loop(0, whole, body, 0)
        if units % pane:
            tile(whole * pane, units % pane)

    def gate_only(slot):
        gate_up(slot, sent, kinds=(0,))

    def last_up(slot, spans, final):
        gate_up(slot, spans, final=final, kinds=(1,))

    half = tall // 2
    near, theirs, paired = ((0, half),), ((half, own),), ((half + own, own),)
    far, direct = ((half, half),), ((own, own),)
    sent, held = ((own, half),), ((0, own), (tall - own, own))

    panes = [(slot, other) for slot in range(4) for other in range(2)]
    pair_first = (3,)

    def pane_of(i):
        slot, other = panes[i]
        return z_of[2][slot] * SIDE + (1 - y if other else y)

    whole_rows = {0: pl.ds(0, own), 1: pl.ds(own, own)}

    def first_hop(i, relayed):
        j = pane_of(i)
        device = to_pair if i in pair_first else to_x
        taken = whole_rows[relayed]
        return remote(
            x_out.at[j, taken, :], x_in.at[j, taken, :], rx_s.at[0], rx_r.at[i, relayed], device
        )

    def second_hop(i):
        j = pane_of(i)
        device = to_x if i in pair_first else to_pair
        return remote(z_out.at[j], z_in.at[j], rz_s.at[0], rz_r.at[j], device)

    def down_sent(i):
        j = pane_of(i)
        x_out[j] = jnp.dot(
            hid[pl.ds(0, half), :], dn[j], preferred_element_type=jnp.float32
        ).astype(jnp.bfloat16)
        first_hop(i, 1).start()

    def down_half(i, relayed):
        j = pane_of(i)
        taken = whole_rows[relayed]
        x_out[j, taken, :] = jnp.dot(
            hid[taken, :], dn[j], preferred_element_type=jnp.float32
        ).astype(jnp.bfloat16)
        first_hop(i, relayed).start()

    def down_held(i):
        j = pane_of(i)
        part[j] = jnp.dot(hid[pl.ds(half, half), :], dn[j], preferred_element_type=jnp.float32)

    def down_both(i):
        j = pane_of(i)
        partial = jnp.dot(hid[...], dn[j], preferred_element_type=jnp.float32)
        x_out[j, whole_rows[0], :] = partial[3 * own :, :].astype(jnp.bfloat16)
        x_out[j, whole_rows[1], :] = partial[own : 2 * own, :].astype(jnp.bfloat16)
        first_hop(i, 1).start()
        part[j, whole_rows[0], :] = partial[2 * own : 3 * own, :]
        part[j, whole_rows[1], :] = partial[:own, :]

    def send_rest(*given):
        for i in given:
            first_hop(i, 0).start()

    def relay(i):
        j = pane_of(i)
        first_hop(i, 1).wait_recv()
        z_out[j] = (part[j, whole_rows[1], :] + x_in[j, whole_rows[1], :].astype(jnp.float32)).astype(
            jnp.bfloat16
        )
        second_hop(i).start()

    def store(i):
        at_cols = pl.ds(pl.multiple_of(pane_of(i) * pane, pane), pane)
        return pltpu.make_async_copy(out_v.at[:, at_cols], out_ref.at[:, at_cols], out_sem.at[0])

    def finish(i):
        j = pane_of(i)
        first_hop(i, 0).wait_recv()
        second_hop(i).wait_recv()
        at_cols = pl.ds(pl.multiple_of(j * pane, pane), pane)
        summed = part[j, whole_rows[0], :] + x_in[j, whole_rows[0], :].astype(jnp.float32)
        out_v[:, at_cols] = (mid[:, at_cols] + (summed + z_in[j].astype(jnp.float32))).astype(
            jnp.bfloat16
        )
        store(i).start()

    def tok_forward(i):
        tok_z[i].wait_recv()
        tok_on[i].start()

    def tok_wait(group):
        for copy in group:
            copy.wait_recv()

    def late_down(dest):
        z_send(2, dest).start()

    def own_down():
        y_send(2, 0).start()

    def apart(ends, mids):
        for want, listed in ((0, ends), (1, mids)):

            @pl.when(is_mid == want)
            def _():
                run(listed)

    def kept_wait(kind):
        kept[kind].wait()

    def settle():
        for copy in halo:
            copy.wait_send()
        for where, semaphore in (
            (att_out, own_s),
            (tok.at[pl.ds(0, 3 * own), :], tok_s),
            (gu.at[0, pl.ds(0, 9 * depth), :], wz_s),
            (gu.at[0, pl.ds(0, 12 * depth), :], wy_s),
            (gu.at[:, pl.ds(0, 12 * depth), :], wc_s),
        ):
            remote(where, where, semaphore.at[0], halo_r.at[0], to_x).wait_send()

    def z_late(*kinds):
        for kind in kinds:
            z_in_and_on(kind, 3)

    def y_late(*kinds):
        for kind in kinds:
            y_in_and_on(kind, 3)

    steps = (
        (y_in_and_on, 0, 0),
        (z_in_and_on, 0, 1),
        (y_in_and_on, 1, 0),
        (z_in_and_on, 1, 1),
        (y_in_and_on, 0, 1),
        (
            apart,
            ((z_in_and_on, 0, 2), (y_in_and_on, 1, 1), (z_in_and_on, 1, 2)),
            ((tok_forward, 0), (y_in_and_on, 1, 1), (own_down,), (tok_forward, 1), (z_in_and_on, 0, 2)),
        ),
        (tok_wait, tok_x),
        (kept_wait, 0),
        (kept_wait, 1),
        (ready_rows, 0),
        (gate_up, 0, near, True),
        (apart, (), ((z_late, 3, 4),)),
        (ready_rows, 1),
        (gate_up, 1, near),
        (
            apart,
            (
                (y_in_and_on, 0, 2),
                (tok_forward, 0),
                (own_down,),
                (y_in_and_on, 1, 2),
                (tok_forward, 1),
            ),
            ((z_late, 5, 6), (z_in_and_on, 1, 2)),
        ),
        (gate_up, 0, paired, True),
        (
            apart,
            ((ready_rows, 2), (gate_up, 2, near), (z_late, 3, 4)),
            ((z_late, 7, 8), (y_in_and_on, 0, 2)),
        ),
        (gate_up, 1, paired),
        (
            apart,
            ((z_late, 5), (gate_up, 2, paired), (z_late, 6, 7)),
            ((z_late, 9, 10), (y_late, 3, 4)),
        ),
        (tok_wait, tok_on),
        (gate_up, 0, theirs, True),
        (apart, ((z_late, 8), (y_late, 3, 4)), ((y_late, 5, 6),)),
        (gate_up, 1, theirs),
        (
            apart,
            ((z_late, 9), (y_late, 5, 6), (z_late, 10), (gate_up, 2, theirs), (ready_gate,), (gate_only, 3)),
            (
                (late_down, 2),
                (y_in_and_on, 1, 2),
                (ready_gate,),
                (gate_only, 3),
                (ready_rows, 2),
                (gate_up, 2, near),
                (late_down, 0),
                (y_late, 7, 8),
                (gate_up, 2, far),
            ),
        ),
        (apart, ((y_late, 7, 8),), ()),
        (y_in_and_on, 2, 0),
        (y_late, 9, 10),
        (ready_up,),
        (z_in_and_on, 2, 1),
        (last_up, 3, direct, 0),
        (apart, ((late_down, 1), (late_down, 2)), ()),
        (kept_wait, 2),
        (ready_down, 0),
        (down_half, 0, 0),
        (last_up, 3, theirs, own),
        (down_half, 0, 1),
        (down_sent, 1),
        (send_rest, 1),
        (gate_up, 3, held, False, half),
        (z_in_and_on, 2, 2),
        (down_held, 0),
        (y_in_and_on, 2, 1),
        (down_held, 1),
        (ready_down, 1),
        (down_sent, 2),
        (send_rest, 2),
        (down_both, 3),
        (send_rest, 3),
        (relay, 0),
        (relay, 1),
        (apart, (), ((z_in_and_on, 2, 3),)),
        (y_in_and_on, 2, 2),
        (ready_down, 2),
        (down_sent, 4),
        (send_rest, 4),
        (apart, ((z_in_and_on, 2, 3),), ()),
        (down_sent, 5),
        (send_rest, 5),
        (down_held, 2),
        (relay, 2),
        (relay, 3),
        (y_in_and_on, 2, 3),
        (ready_down, 3),
        (down_sent, 6),
        (down_sent, 7),
        (send_rest, 6, 7),
        (down_held, 4),
        (relay, 4),
        (down_held, 5),
        (down_held, 6),
        (relay, 5),
        (down_held, 7),
        (settle,),
        (relay, 6),
        (relay, 7),
        (finish, 0),
        (finish, 1),
        (finish, 2),
        (finish, 3),
        (finish, 4),
        (finish, 5),
        (finish, 6),
        (finish, 7),
    )

    def run(listed):
        for action, *given in listed:
            if action is apart:
                apart(*given)
                continue
            action(*given)

    run(steps)

    remote(x_out, x_out, rx_s.at[0], halo_r.at[0], to_x).wait_send()
    remote(z_out, z_out, rz_s.at[0], halo_r.at[0], to_x).wait_send()
    pltpu.make_async_copy(out_v, out_ref, out_sem.at[0]).wait()


def one_kernel(
    resid, queries, keys, values, documents, sinks, out_proj, norm_gain, gate_proj, up_proj, down_proj
):
    rows, own, width = queries.shape[0], resid.shape[0], resid.shape[1]
    units = gate_proj.shape[1] // 2
    deep = gate_proj.shape[0] * CHAIN * SIDE * CORES
    pane = gate_proj.shape[0] * CORES
    panes = width // pane
    heads_cols, kv_cols = queries.shape[1], keys.shape[1]
    bf16, f32 = jnp.bfloat16, jnp.float32
    anywhere = pl.BlockSpec(memory_space=pl.ANY)
    dma = pltpu.SemaphoreType.DMA
    tall = 4 * own
    return pl.pallas_call(
        layer_kernel,
        out_shape=jax.ShapeDtypeStruct((own, width), bf16),
        in_specs=[anywhere] * 11,
        out_specs=anywhere,
        scratch_shapes=[
            pltpu.VMEM((rows // WINDOW, WINDOW), jnp.int32),
            pltpu.VMEM((1, width), f32),
            pltpu.SMEM((1, sinks.shape[0]), f32),
            pltpu.VMEM((own, width), bf16),
            pltpu.VMEM((rows, heads_cols), bf16),
            pltpu.VMEM((rows + WINDOW, kv_cols), bf16),
            pltpu.VMEM((rows + WINDOW, kv_cols), bf16),
            pltpu.VMEM((1, WINDOW), jnp.int32),
            pltpu.VMEM((own, width), bf16),
            pltpu.VMEM(out_proj.shape, bf16),
            pltpu.VMEM((own, out_proj.shape[0]), bf16),
            pltpu.VMEM((own, heads_cols), bf16),
            pltpu.VMEM((own, width), f32),
            pltpu.VMEM((tall, width), bf16),
            pltpu.VMEM((2, deep, units), bf16),
            pltpu.VMEM((panes, units, pane), bf16),
            pltpu.VMEM((2, tall, units), f32),
            pltpu.VMEM((tall, units), bf16),
            pltpu.VMEM((panes, tall // 2, pane), f32),
            pltpu.VMEM((panes, tall // 2, pane), bf16),
            pltpu.VMEM((panes, tall // 2, pane), bf16),
            pltpu.VMEM((panes, own, pane), bf16),
            pltpu.VMEM((panes, own, pane), bf16),
            dma((8,)),
            dma((3,)),
            dma((3,)),
            dma((1,)),
            dma((own // WINDOW,)),
            dma((1,)),
            dma((3, 2)),
            dma((3,)),
            dma((1,)),
            dma((15,)),
            dma((1,)),
            dma((18,)),
            dma((1,)),
            dma((9,)),
            dma((1,)),
            dma((panes, 2)),
            dma((1,)),
            dma((panes,)),
            dma((1,)),
        ],
        compiler_params=pltpu.CompilerParams(
            collective_id=0, has_side_effects=True, vmem_limit_bytes=66_000_000
        ),
        name="layer",
    )(
        documents.reshape(rows // WINDOW, WINDOW),
        norm_gain.reshape(1, width),
        sinks.reshape(1, sinks.shape[0]),
        resid,
        queries,
        keys,
        values,
        out_proj,
        gate_proj,
        up_proj,
        down_proj,
    )


def solution(mesh):
    in_specs = (
        P(("sp", "tp"), None),
        P("sp", "tp"),
        P("sp", "tp"),
        P("sp", "tp"),
        P("sp"),
        P("tp"),
        P(),
        P(),
        P("sp", "tp"),
        P("sp", "tp"),
        P("tp", "sp"),
    )
    out_specs = P(("sp", "tp"), None)
    if fits(mesh):
        program = lambda *arrays: one_kernel(*arrays)
        return jax.shard_map(
            program, mesh=mesh, in_specs=in_specs, out_specs=out_specs, check_vma=False
        )
    return jax.shard_map(shards, mesh=mesh, in_specs=in_specs, out_specs=out_specs, check_vma=False)
```
